256 devices in a mesh: ep: 64 (over z, y, core), tp: 4 (over x).
Axes of the slice: x: 4, y: 4, z: 8, core: 2. Of those that a mesh axis runs over, the one named last changes fastest.
Arguments:
- queries: bfloat16 [16384, 1536], P('ep', 'tp'), may hold values from -6 to 6
- kv_latent: bfloat16 [16384, 512], P('ep'), may hold values from -6 to 6
- rope_key: bfloat16 [16384, 64], P('ep'), may hold values from -6 to 6
- latent_gain: float32 [512], replicated, may hold values from 0.1 to 1.9
- w_key_up: bfloat16 [512, 1024], P(None, 'tp'), may hold values from -0.25 to 0.25
- w_value_up: bfloat16 [512, 1024], P(None, 'tp'), may hold values from -0.25 to 0.25
- query_gain: float32 [192], replicated, may hold values from 0.1 to 1.9
- key_gain: float32 [128], replicated, may hold values from 0.1 to 1.9
- rope_gain: float32 [64], replicated, may hold values from 0.1 to 1.9
- out_gain: float32 [128], replicated, may hold values from 0.1 to 1.9
- moe_tokens: bfloat16 [16384, 2048], P('ep'), may hold values from -6 to 6
- moe_gain: float32 [2048], replicated, may hold values from 0.1 to 1.9
- routes: int32 [16384, 2], P('ep'), may hold values from 0 to 63, all different within a row; in each aligned block of 64 rows (0 to 63, 64 to 127, ...) at most 3 rows name the same one
- route_weights: float32 [16384, 2], P('ep'), may hold values from 0.25 to 1
- w_gate: bfloat16 [64, 2048, 3584], P('ep', None, 'tp'), may hold values from -0.125 to 0.125
- w_up: bfloat16 [64, 2048, 3584], P('ep', None, 'tp'), may hold values from -0.125 to 0.125
- w_down: bfloat16 [64, 3584, 2048], P('ep', 'tp'), may hold values from -0.09375 to 0.09375
Outputs:
- attended: bfloat16 [16384, 1024], P('ep', 'tp')
- moe_out: bfloat16 [16384, 2048], P(('ep', 'tp'))
The draws below stay inside these ranges and needn't reach their ends.
Inputs may be any that keep to these rules, and one draw needn't show every extreme that they name: `routes`: each row names 2 different experts of 0 to 63; in each aligned block of 64 rows no expert is named by more than 3 rows, and in some block one expert is named by exactly 3.
All inputs are finite; a program needn't handle non-finite values.
Results may differ from the reference program's by a relative error of at most 0.0071.
Values may be sent and summed in bfloat16 or wider, within the bound.
A program may use at most 128 MiB of HBM per device.

```python
import math
import jax
import jax.numpy as jnp
import numpy as np
from jax import lax

D = 2048
HEADS = 8
NOPE = 128
ROPE_DIM = 64
VHEAD = 128
LATENT = 512
FF = 3584
TOP = 2
EXPERTS = 64
SEQ = 16384
MOE_ROWS = 16384
Q_ROWS = 64
CAP = 3


def shard_levels(stream_key, extent, shards, least, largest):
    def one(dim, parts):
        heights = jax.random.uniform(jax.random.fold_in(jax.random.fold_in(stream_key, 6), dim), (parts,), jnp.float32, least / len(shards), largest / len(shards))
        return jnp.repeat(jnp.exp(heights), extent[dim] // parts).reshape((-1,) + (1,) * (len(extent) - dim - 1))

    level = one(*shards[0])
    for cut in shards[1:]:
        level = level * one(*cut)
    return level


def assign_block(key, own, number, rows, count, top, bound, lean):
    order = jax.random.permutation(key, count)
    heavy_load, ordinary = portions_of(count, rows * top, bound, lean, True), portions_of(count, rows * top, bound, lean, False)
    places = jnp.arange(count)

    def named(tallies, offset_by):
        used = int((tallies > 0).sum())
        fixed = max(1, used // 4)
        shifted = fixed + (places - fixed + offset_by * (used - fixed)) % max(1, count - fixed)
        return jnp.zeros((count,), jnp.int32).at[order[jnp.where(places < fixed, places, shifted)]].set(jnp.asarray(tallies, jnp.int32))

    tallies = jnp.where(number % 4 == 0, named(heavy_load, number // 4), named(ordinary, number - number // 4 - 1))
    mixed = jax.random.permutation(jax.random.fold_in(own, 3), count)
    giver, receiver = mixed[0:count // 2 * 2:2], mixed[1:count // 2 * 2:2]
    margin = jnp.minimum(tallies[giver] - 1, bound - tallies[receiver]) // 2
    margin = jnp.where((giver == order[0]) | (receiver == order[0]) | (tallies[receiver] == 0), 0, jnp.maximum(margin, 0))
    shifted = jax.random.randint(jax.random.fold_in(own, 4), (count // 2,), 0, 1 << 20) % (margin + 1)
    tallies = tallies.at[giver].add(-shifted).at[receiver].add(shifted)
    labels = jnp.searchsorted(jnp.cumsum(tallies), jnp.arange(rows * top), side="right").astype(jnp.int32)
    table = labels.reshape(top, rows).T
    table = table[jax.random.permutation(jax.random.fold_in(own, 1), rows)]
    offset_by = jax.random.randint(jax.random.fold_in(own, 2), (rows, 1), 0, top)
    return jnp.take_along_axis(table, (jnp.arange(top)[None, :] + offset_by) % top, axis=1)


def portions_of(number_of, total, most, skew, full):
    portions = [(1 << 20) // math.isqrt(standing ** skew) + 1 for standing in range(1, number_of + 1)]
    largest = most if full else min(most, max(-(-total // number_of), total * portions[0] // sum(portions)))
    least = 1 if total - largest >= number_of - 1 else 0
    given, surplus = [largest] + [least] * (number_of - 1), total - largest - least * (number_of - 1)
    while surplus > 0:
        movable = [i for i in range(1, number_of) if given[i] < largest] or [i for i in range(1, number_of) if given[i] < most]
        mass, remaining = sum([portions[i] for i in movable]), surplus
        for i in movable:
            addition = min(most - given[i], max(1, remaining * portions[i] // mass), surplus)
            given[i] = given[i] + addition
            surplus = surplus - addition
    return np.array(given)


def scatter_about(stream_key, dims, scale, limit, shards=(), held_as=jnp.bfloat16):
    drawn = scale * jax.random.normal(stream_key, dims, jnp.float32)
    if shards:
        drawn = drawn * shard_levels(stream_key, dims, shards, -0.22, 0.18)
    return jnp.clip(drawn, -limit, limit).astype(held_as)


def setup_inputs(seed: int = 0) -> dict:
    streams_of = jax.random.split(jax.random.key(seed), 18)
    queries = scatter_about(streams_of[0], (SEQ, HEADS * (NOPE + ROPE_DIM)), 1.0, 6.0, ((0, 64), (1, 4)))
    kv_latent = scatter_about(streams_of[1], (SEQ, LATENT), 1.0, 6.0, ((0, 64),))
    rope_key = scatter_about(streams_of[2], (SEQ, ROPE_DIM), 1.0, 6.0, ((0, 64),))
    latent_gain = jnp.clip(1.0 + 0.18 * jax.random.normal(streams_of[3], (LATENT,), jnp.float32), 0.1, 1.9)
    w_key_up = scatter_about(streams_of[4], (LATENT, HEADS * NOPE), LATENT ** -0.5, 0.25, ((1, 4),))
    w_value_up = scatter_about(streams_of[5], (LATENT, HEADS * VHEAD), LATENT ** -0.5, 0.25, ((1, 4),))
    query_gain = jnp.clip(1.0 + 0.18 * jax.random.normal(streams_of[6], (NOPE + ROPE_DIM,), jnp.float32), 0.1, 1.9)
    key_gain = jnp.clip(1.0 + 0.18 * jax.random.normal(streams_of[7], (NOPE,), jnp.float32), 0.1, 1.9)
    rope_gain = jnp.clip(1.0 + 0.18 * jax.random.normal(streams_of[8], (ROPE_DIM,), jnp.float32), 0.1, 1.9)
    out_gain = jnp.clip(1.0 + 0.18 * jax.random.normal(streams_of[9], (VHEAD,), jnp.float32), 0.1, 1.9)
    moe_tokens = scatter_about(streams_of[10], (MOE_ROWS, D), 1.0, 6.0, ((0, 64),))
    moe_gain = jnp.clip(1.0 + 0.18 * jax.random.normal(streams_of[11], (D,), jnp.float32), 0.1, 1.9)
    routes_keys = jax.random.split(jax.random.fold_in(streams_of[12], 1), MOE_ROWS // Q_ROWS)
    routes_turns = jax.random.permutation(jax.random.fold_in(streams_of[12], 3), MOE_ROWS // Q_ROWS)
    routes = jax.vmap(lambda own, number: assign_block(jax.random.fold_in(streams_of[12], 2), own, number, Q_ROWS, EXPERTS, TOP, CAP, 1))(routes_keys, routes_turns).reshape((MOE_ROWS, TOP))
    route_weights = jnp.clip(0.25 + 0.75 * jax.random.uniform(streams_of[13], (MOE_ROWS, TOP), jnp.float32) ** shard_levels(streams_of[13], (MOE_ROWS, TOP), ((0, 64),), -0.2, 0.2), 0.25, 1.0)
    w_gate = scatter_about(streams_of[14], (EXPERTS, D, FF), D ** -0.5, 0.125, ((0, 64), (2, 4)))
    w_up = scatter_about(streams_of[15], (EXPERTS, D, FF), D ** -0.5, 0.125, ((0, 64), (2, 4)))
    w_down = scatter_about(streams_of[16], (EXPERTS, FF, D), FF ** -0.5, 0.09375, ((0, 64), (1, 4)))
    return {"queries": queries, "kv_latent": kv_latent, "rope_key": rope_key, "latent_gain": latent_gain, "w_key_up": w_key_up, "w_value_up": w_value_up, "query_gain": query_gain, "key_gain": key_gain, "rope_gain": rope_gain, "out_gain": out_gain, "moe_tokens": moe_tokens, "moe_gain": moe_gain, "routes": routes, "route_weights": route_weights, "w_gate": w_gate, "w_up": w_up, "w_down": w_down}


EPS = 1e-06
THETA = 500000.0

def rms_norm(values, norm_gain):
    return values * lax.rsqrt(lax.optimization_barrier(jnp.mean(values * values, axis=-1, keepdims=True)) + EPS) * norm_gain

def rounded(values):
    return lax.optimization_barrier(values.astype(jnp.bfloat16))

def rope_tables(positions, rope_dim):
    freqs = 1.0 / THETA ** (jnp.arange(0, rope_dim, 2, dtype=jnp.float32) / rope_dim)
    angles = positions.astype(jnp.float32)[:, None] * freqs[None, :]
    return (jnp.cos(angles), jnp.sin(angles))

def rotate(values, rot_cos, rot_sin):
    half_dim = values.shape[-1] // 2
    first_half = values[..., :half_dim]
    second_half = values[..., half_dim:]
    return jnp.concatenate([first_half * rot_cos - second_half * rot_sin, second_half * rot_cos + first_half * rot_sin], axis=-1)

def attention(queries, kv_latent, rope_key, latent_gain, w_key_up, w_value_up, query_gain, key_gain, rope_gain, out_gain):
    seq_len = queries.shape[0]
    positions = jnp.arange(seq_len, dtype=jnp.int32)
    rot_cos, rot_sin = rope_tables(positions, ROPE_DIM)
    latent = rounded(rms_norm(kv_latent.astype(jnp.float32), latent_gain))
    key_nope = jnp.dot(latent, w_key_up, preferred_element_type=jnp.float32).reshape(seq_len, HEADS, NOPE)
    key_nope = rounded(rms_norm(key_nope, key_gain)).astype(jnp.float32)
    values = rounded(jnp.dot(latent, w_value_up, preferred_element_type=jnp.float32))
    values = values.astype(jnp.float32).reshape(seq_len, HEADS, VHEAD)
    rot_key = rounded(rotate(rms_norm(rope_key.astype(jnp.float32), rope_gain), rot_cos, rot_sin)).astype(jnp.float32)
    query = rms_norm(queries.astype(jnp.float32).reshape(seq_len, HEADS, NOPE + ROPE_DIM), query_gain)
    query_nope = rounded(query[..., :NOPE]).astype(jnp.float32)
    query_rope = rounded(rotate(query[..., NOPE:], rot_cos[:, None, :], rot_sin[:, None, :])).astype(jnp.float32)
    scale = (NOPE + ROPE_DIM) ** (-0.5)
    block_rows = math.gcd(seq_len, 512)

    def one_block(block_index):
        block_first = block_index * block_rows
        q_nope = lax.dynamic_slice_in_dim(query_nope, block_first, block_rows, 0)
        q_rope = lax.dynamic_slice_in_dim(query_rope, block_first, block_rows, 0)
        scores = (jnp.einsum('qhd,khd->hqk', q_nope, key_nope, precision=lax.Precision.HIGHEST) + jnp.einsum('qhr,kr->hqk', q_rope, rot_key, precision=lax.Precision.HIGHEST)) * scale
        query_pos = block_first + jnp.arange(block_rows, dtype=jnp.int32)
        visible = (query_pos[:, None] >= positions[None, :])[None]
        exp_scores = jnp.where(visible, jnp.exp(scores), 0.0)
        denominator = lax.optimization_barrier(jnp.sum(exp_scores, axis=-1))
        weighted = jnp.einsum('hqk,khd->qhd', rounded(exp_scores).astype(jnp.float32), values, precision=lax.Precision.HIGHEST)
        mixed = weighted / jnp.transpose(denominator)[:, :, None]
        return rms_norm(mixed, out_gain).astype(jnp.bfloat16).reshape(block_rows, HEADS * VHEAD)
    blocks = lax.map(one_block, jnp.arange(seq_len // block_rows, dtype=jnp.int32))
    return blocks.reshape(seq_len, HEADS * VHEAD)

def experts_layer(moe_tokens, moe_gain, routes, route_weights, w_gate, w_up, w_down):
    n_rows = moe_tokens.shape[0]
    normed = rounded(rms_norm(moe_tokens.astype(jnp.float32), moe_gain))
    n_blocks = n_rows // Q_ROWS
    assigned = Q_ROWS * TOP
    slot_count = EXPERTS * CAP
    chosen = routes.reshape(n_blocks, assigned)
    onehot = (chosen[..., None] == jnp.arange(EXPERTS, dtype=jnp.int32)).astype(jnp.int32)
    rank = lax.optimization_barrier(jnp.sum((jnp.cumsum(onehot, axis=1) - onehot) * onehot, axis=-1)).astype(jnp.int32)
    slots = chosen * CAP + rank
    row_ids = jnp.arange(n_blocks, dtype=jnp.int32)[:, None] * Q_ROWS + jnp.arange(assigned, dtype=jnp.int32)[None, :] // TOP
    slot_hit = (slots[..., None] == jnp.arange(slot_count, dtype=jnp.int32)).astype(jnp.int32)
    table = lax.optimization_barrier(jnp.sum(slot_hit * (row_ids[..., None] + 1), axis=1)) - 1
    table = jnp.where(table < 0, n_rows, table).astype(jnp.int32)
    padded = jnp.concatenate([normed, jnp.zeros((1, normed.shape[1]), jnp.bfloat16)], axis=0)

    def one_expert(expert):
        rows_used = lax.dynamic_slice_in_dim(table, expert * CAP, CAP, 1).reshape(-1)
        inputs = padded[rows_used]
        gate = jnp.dot(inputs, w_gate[expert], preferred_element_type=jnp.float32)
        upward = jnp.dot(inputs, w_up[expert], preferred_element_type=jnp.float32)
        hidden = (jax.nn.silu(gate) * upward).astype(jnp.bfloat16)
        return rounded(jnp.dot(hidden, w_down[expert], preferred_element_type=jnp.float32))
    outputs = lax.map(one_expert, jnp.arange(EXPERTS, dtype=jnp.int32))
    place = jnp.arange(n_blocks, dtype=jnp.int32)[:, None] * CAP + rank
    picked = outputs[chosen, place].astype(jnp.float32)
    scaled = picked * route_weights.reshape(n_blocks, assigned)[..., None]
    mixed = lax.optimization_barrier(jnp.sum(scaled.reshape(n_rows, TOP, picked.shape[-1]), axis=1))
    return mixed.astype(jnp.bfloat16)

def reference(queries, kv_latent, rope_key, latent_gain, w_key_up, w_value_up, query_gain, key_gain, rope_gain, out_gain, moe_tokens, moe_gain, routes, route_weights, w_gate, w_up, w_down):
    attended = attention(queries, kv_latent, rope_key, latent_gain, w_key_up, w_value_up, query_gain, key_gain, rope_gain, out_gain)
    moe_out = experts_layer(moe_tokens, moe_gain, routes, route_weights, w_gate, w_up, w_down)
    return (attended, moe_out)
```

```python
import functools
import math

import jax
import jax.numpy as jnp
import numpy as np
from jax import lax
from jax.experimental import pallas as pl
from jax.experimental.pallas import tpu as pltpu
from jax.sharding import Mesh
from jax.sharding import PartitionSpec as P

BF, F32, I32 = jnp.bfloat16, jnp.float32, jnp.int32
MESH = pl.DeviceIdType.MESH

EP = ("ep_0", "ep_1", "ep_2")
EP_TP = ("ep_0", "ep_1", "ep_2", "tp")


EPS = 1e-06
THETA = 500000.0


def side_by_side(arrays, axis, dim, along):
    widths = [a.shape[along] for a in arrays]
    both = jnp.concatenate(arrays, axis=along)
    whole = lax.all_gather(both, axis, axis=dim, tiled=True)
    return tuple(jnp.split(whole, [sum(widths[:k]) for k in range(1, len(widths))], axis=along))


def in_blocks(x, dim, count):
    dims = x.shape
    blocks = x.reshape(*dims[:dim], count, dims[dim] // count, *dims[dim + 1 :])
    return jnp.moveaxis(blocks, dim, 0)


def summed_on_arrival(x, axis, dim):
    count = lax.axis_size(axis)
    blocks = lax.all_to_all(in_blocks(x, dim, count), axis, 0, 0, tiled=True)
    return jnp.sum(blocks, axis=0)


def joined_along(blocks, dim):
    blocks = jnp.moveaxis(blocks, 0, dim)
    dims = blocks.shape
    return blocks.reshape(*dims[:dim], dims[dim] * dims[dim + 1], *dims[dim + 2 :])


def moved_by_axis(blocks, axes, order):
    dims = [lax.axis_size(a) for a in axes]
    blocks = blocks.reshape(*dims, *blocks.shape[1:])
    for k in order:
        blocks = lax.all_to_all(blocks, axes[k], split_axis=k, concat_axis=k, tiled=True)
    return blocks.reshape(-1, *blocks.shape[len(axes) :])


def core_and_chips(x, groups, order, split_dim, concat_dim):
    count = lax.axis_size(groups[0]) * lax.axis_size(groups[1])
    blocks = in_blocks(x, split_dim, count)
    return joined_along(moved_by_axis(blocks, groups, order), concat_dim)


def rms_norm(values, norm_gain):
    return values * lax.rsqrt(jnp.mean(values * values, axis=-1, keepdims=True) + EPS) * norm_gain


def rope_tables(positions, rope_dim):
    freqs = 1.0 / THETA ** (jnp.arange(0, rope_dim, 2, dtype=jnp.float32) / rope_dim)
    angles = positions.astype(jnp.float32)[:, None] * freqs[None, :]
    return (jnp.cos(angles), jnp.sin(angles))


def rotate(values, rot_cos, rot_sin):
    half_dim = values.shape[-1] // 2
    first_half = values[..., :half_dim]
    second_half = values[..., half_dim:]
    return jnp.concatenate(
        [
            first_half * rot_cos - second_half * rot_sin,
            second_half * rot_cos + first_half * rot_sin,
        ],
        axis=-1,
    )


def attention_part(
    queries,
    kv_latent,
    rope_key,
    latent_gain,
    w_key_up,
    w_value_up,
    query_gain,
    key_gain,
    rope_gain,
    out_gain,
):
    tok_rows = queries.shape[0]
    nope_dim = key_gain.shape[0]
    value_dim = out_gain.shape[0]
    rope_dim = rope_key.shape[1]
    head_count = w_key_up.shape[1] // nope_dim
    offset = lax.axis_index(EP) * tok_rows
    positions = offset + jnp.arange(tok_rows, dtype=jnp.int32)
    rot_cos, rot_sin = rope_tables(positions, rope_dim)
    latent = rms_norm(kv_latent.astype(jnp.float32), latent_gain).astype(jnp.bfloat16)
    key_nope = jnp.dot(latent, w_key_up, preferred_element_type=jnp.float32).reshape(
        tok_rows, head_count, nope_dim
    )
    key_nope = (
        rms_norm(key_nope, key_gain).astype(jnp.bfloat16).reshape(tok_rows, head_count * nope_dim)
    )
    values = jnp.dot(latent, w_value_up, preferred_element_type=jnp.float32).astype(jnp.bfloat16)
    rot_key = rotate(rms_norm(rope_key.astype(jnp.float32), rope_gain), rot_cos, rot_sin).astype(
        jnp.bfloat16
    )
    keys_values = jnp.concatenate([key_nope, values], axis=1)
    query = rms_norm(
        queries.astype(jnp.float32).reshape(tok_rows, head_count, nope_dim + rope_dim), query_gain
    )
    query_nope = query[..., :nope_dim].astype(jnp.bfloat16)
    query_rope = rotate(query[..., nope_dim:], rot_cos[:, None, :], rot_sin[:, None, :]).astype(
        jnp.bfloat16
    )
    scale = (nope_dim + rope_dim) ** (-0.5)
    last_pos = offset + tok_rows - 1
    initial = (
        jnp.zeros((tok_rows, head_count, value_dim), jnp.float32),
        jnp.zeros((head_count, tok_rows), jnp.float32),
    )
    totals = initial
    key_piece, rope_piece = side_by_side((keys_values, rot_key), EP, 0, 1)
    piece_rows = key_piece.shape[0]
    block_rows = math.gcd(piece_rows, 512)

    def one_block(totals_in, block_index):
        block_first = block_index * block_rows
        kv_block = lax.dynamic_slice_in_dim(key_piece, block_first, block_rows, 0)
        rope_block = lax.dynamic_slice_in_dim(rope_piece, block_first, block_rows, 0)

        def attend(sums_in):
            weighted, denominator = sums_in
            key_block = kv_block[:, : head_count * nope_dim].reshape(
                block_rows, head_count, nope_dim
            )
            value_block = kv_block[:, head_count * nope_dim :].reshape(
                block_rows, head_count, value_dim
            )
            scores = (
                jnp.einsum(
                    "qhd,khd->hqk", query_nope, key_block, preferred_element_type=jnp.float32
                )
                + jnp.einsum(
                    "qhr,kr->hqk", query_rope, rope_block, preferred_element_type=jnp.float32
                )
            ) * scale
            key_pos = block_first + jnp.arange(block_rows, dtype=jnp.int32)
            visible = (positions[:, None] >= key_pos[None, :])[None]
            exp_scores = jnp.where(visible, jnp.exp(scores), 0.0)
            denominator = denominator + jnp.sum(exp_scores, axis=-1)
            weighted = weighted + jnp.einsum(
                "hqk,khd->qhd",
                exp_scores.astype(jnp.bfloat16),
                value_block,
                preferred_element_type=jnp.float32,
            )
            return (weighted, denominator)

        def unchanged(sums_in):
            return sums_in

        return (lax.cond(block_first <= last_pos, attend, unchanged, totals_in), None)

    totals, _ = lax.scan(one_block, totals, jnp.arange(piece_rows // block_rows, dtype=jnp.int32))
    weighted, denominator = totals
    mixed = weighted / jnp.transpose(denominator)[:, :, None]
    return rms_norm(mixed, out_gain).astype(jnp.bfloat16).reshape(tok_rows, head_count * value_dim)


SRC = 8
MSG = 16
CAP = 12


def split_two(v):
    hi = v.astype(BF)
    return hi, (v - hi.astype(F32)).astype(BF)


def fixed_selects():
    packed = np.arange(16 * MSG)
    slot = np.arange(16 * CAP)
    src, s = slot // CAP, slot % CAP
    main = (src * MSG + s)[:, None] == packed[None, :]
    extra = [((src * MSG + CAP + s % 4)[:, None] == packed[None, :]) & (s // 4 == j)[:, None] for j in range(3)]
    unpack_extra = np.concatenate(extra, axis=1)
    pack_extra = np.concatenate([e.T for e in extra], axis=0)
    return [jnp.asarray(a.astype(np.float32), BF) for a in (main, unpack_extra, main.T, pack_extra)]


class Place:
    def __init__(self, n_z):
        self.n_z = n_z
        self.z = lax.axis_index("ep_0")
        self.y = lax.axis_index("ep_1")
        self.c = lax.axis_index("ep_2")
        self.t = lax.axis_index("tp")
        self.s8 = self.y * 2 + self.c

    def row(self, order):
        up = order % 2
        return up * ((order + 1) // 2) + (1 - up) * ((self.n_z - order // 2) % self.n_z)

    def x(self, step):
        return (self.z, self.y, self.c, (self.t + step) % 4)

    def at(self, z, s8):
        return (z, s8 // 2, s8 % 2, self.t)


def greet(pl_, n_z):
    barrier = pltpu.get_barrier_semaphore()

    def one(i, _):
        z, s = (pl_.z + i // SRC) % n_z, (pl_.s8 + i % SRC) % SRC
        pl.semaphore_signal(barrier, inc=1, device_id=pl_.at(z, s), device_id_type=MESH)
        return 0

    lax.fori_loop(1, n_z * SRC, one, 0)
    for step in (1, 2, 3):
        pl.semaphore_signal(barrier, inc=1, device_id=pl_.x(step), device_id_type=MESH)


def met(n_z):
    pl.semaphore_wait(pltpu.get_barrier_semaphore(), n_z * SRC - 1 + 3)


def remote(src, dst, send, recv, device):
    return pltpu.make_async_remote_copy(
        src_ref=src, dst_ref=dst, send_sem=send, recv_sem=recv, device_id=device, device_id_type=MESH
    )


def await_bytes(ref, sem):
    pltpu.make_async_copy(ref, ref, sem).wait()


def dot(a, b):
    return jnp.dot(a, b, preferred_element_type=F32)


def experts_kernel(
    n_z,
    tokens,
    gain,
    routes,
    routes_t,
    weights,
    un_main,
    un_extra,
    pk_main,
    pk_extra,
    wg_hbm,
    wu_hbm,
    wd_hbm,
    out,
    wg,
    wu,
    wd,
    normed,
    outb,
    arr,
    rows,
    gacc,
    uacc,
    hid,
    wmix,
    far,
    to_r,
    to_l,
    relay,
    from_l,
    from_r,
    retb,
    reti,
    fino,
    fini,
    w_sem,
    own_sem,
    out_sem,
    self_sem,
    xs_sem,
    xr_sem,
    rs_send,
    relay_sem,
    fl_sem,
    fr_sem,
    ret_send,
    ret_sem,
    fin_send,
    fin_sem,
):
    me = Place(n_z)
    greet(me, n_z)
    loads = [
        pltpu.make_async_copy(h.at[0], v, w_sem.at[k]) for k, (h, v) in enumerate(((wg_hbm, wg), (wu_hbm, wu), (wd_hbm, wd)))
    ]
    for load in loads:
        load.start()
    n_rows, model = tokens.shape
    cols = model // 4
    quarter = n_rows // 4

    exp_ids = lax.broadcasted_iota(I32, (64, n_rows), 0)
    ra, rb = routes_t[0:1, :], routes_t[1:2, :]
    hit_a, hit_b = exp_ids == ra, exp_ids == rb
    both = jnp.where(hit_a | hit_b, 1.0, 0.0).astype(BF)
    i0 = lax.broadcasted_iota(I32, (n_rows, n_rows), 0)
    i1 = lax.broadcasted_iota(I32, (n_rows, n_rows), 1)
    same = (i0 // quarter) == (i1 // quarter)
    earlier_t = jnp.where((i0 < i1) & same, 1.0, 0.0).astype(BF)
    count_t = dot(both, earlier_t)
    base_t = lax.broadcasted_iota(I32, (1, n_rows), 1) // quarter * 3

    def places(hit, chosen):
        s = base_t + jnp.sum(jnp.where(hit, count_t, 0.0), axis=0, keepdims=True).astype(I32)
        return chosen * MSG + s, chosen * MSG + CAP + s % 4 + 2048 * (s // 4)

    (ma, xa), (mb, xb) = places(hit_a, ra), places(hit_b, rb)

    v = tokens[...].astype(F32)
    scale = lax.rsqrt(jnp.mean(v * v, axis=-1, keepdims=True) + EPS)
    mine = pl.ds(pl.multiple_of(me.t * cols, cols), cols)
    normed[...] = (tokens[:, mine].astype(F32) * scale * gain[:, mine]).astype(BF)

    met(n_z)

    def dispatch(o, _):
        z = (me.z + me.row(o)) % n_z
        first = z * SRC * MSG
        ids = lax.broadcasted_iota(I32, (SRC * MSG, n_rows), 0) + first
        main = jnp.where((ids == ma) | (ids == mb), 1.0, 0.0).astype(BF)
        block = dot(main, normed[:, : 3 * 128])
        extra = []
        for j in range(3):
            idj = ids + 2048 * j
            sel = jnp.where((idj == xa) | (idj == xb), 1.0, 0.0).astype(BF)
            extra.append(dot(sel, normed[:, 3 * 128 :]))
        block = block + jnp.concatenate(extra, axis=1)
        outb[o] = block.astype(BF).reshape(SRC, MSG, 3 * 128)

        def send(i, _):
            s = (me.s8 + i) % SRC
            remote(outb.at[o, s], arr.at[0, o, me.s8], out_sem, own_sem.at[o], me.at(z, s)).start()
            return 0

        lax.fori_loop(jnp.where(o == 0, 1, 0), SRC, send, 0)
        return 0

    lax.fori_loop(0, n_z, dispatch, 0)
    pltpu.make_async_copy(outb.at[0, me.s8], arr.at[0, 0, me.s8], own_sem.at[0]).start()

    lane_e = lax.broadcasted_iota(I32, (n_rows, 128), 1)
    ca, cb = routes[:, 0:1], routes[:, 1:2]
    on_a, on_b = lane_e == ca, lane_e == cb
    earlier = jnp.where((i1 < i0) & same, 1.0, 0.0).astype(BF)
    count = dot(earlier, jnp.where(on_a | on_b, 1.0, 0.0).astype(BF))
    base = lax.broadcasted_iota(I32, (n_rows, 1), 0) // quarter * 3
    wa, wb = weights[:, 0:1], weights[:, 1:2]

    def places_c(hit, chosen):
        s = base + jnp.sum(jnp.where(hit, count, 0.0), axis=1, keepdims=True).astype(I32)
        return chosen * MSG + s, chosen * MSG + CAP + s % 4 + 2048 * (s // 4)

    (cma, cxa), (cmb, cxb) = places_c(on_a, ca), places_c(on_b, cb)

    def mix(k, _):
        lanes = lax.broadcasted_iota(I32, (n_rows, 64 * MSG), 1)
        idk = lanes + 2048 * (k - 1)
        pa, pb = jnp.where(k == 0, cma - 2048, cxa), jnp.where(k == 0, cmb - 2048, cxb)
        w = jnp.where(idk == pa, wa, 0.0) + jnp.where(idk == pb, wb, 0.0)
        hi, lo = split_two(w)
        wmix[k, 0] = hi
        wmix[k, 1] = lo
        return 0

    lax.fori_loop(0, 4, mix, 0)

    def pass_on(b, o, step, dst):
        remote(arr.at[b, o], arr.at[dst, o], xs_sem.at[b, step % 4 // 2], xr_sem.at[dst - 1, o], me.x(step)).start()

    def unpack(b, p):
        packed = arr[b, pl.ds(2 * p, 2)].reshape(2 * SRC * MSG, 3 * 128)
        tiles = jnp.concatenate([packed[:, 128 * j : 128 * (j + 1)] for j in range(3)], axis=0)
        r = pl.ds(pl.multiple_of(p * 192, 192), 192)
        rows[b, r, : 3 * 128] = dot(un_main[...], packed).astype(BF)
        rows[b, r, 3 * 128 :] = dot(un_extra[...], tiles).astype(BF)

    def gather(o, _):
        await_bytes(arr.at[0, o], own_sem.at[o])
        pass_on(0, o, 1, 1)
        pass_on(0, o, 3, 2)

        @pl.when(o % 2 == 1)
        def _():
            unpack(0, o // 2)

        return 0

    def relay_on(o):
        await_bytes(arr.at[1, o], xr_sem.at[0, o])
        await_bytes(arr.at[2, o], xr_sem.at[1, o])

        @pl.when(o % 2 == 0)
        def _():
            pass_on(1, o, 1, 3)

        @pl.when(o % 2 == 1)
        def _():
            pass_on(2, o, 3, 3)
            unpack(1, o // 2)
            unpack(2, o // 2)

    def gather_step(o, _):
        gather(o, 0)
        relay_on(o - 1)
        return 0

    gather(0, 0)
    lax.fori_loop(1, n_z, gather_step, 0)
    relay_on(n_z - 1)

    loads[0].wait()
    loads[1].wait()
    n_all = rows.shape[1]
    part = 192
    sides = ((0, 0), (1, 3), (2, 1), (3, 2))

    def up_gate(b, rank, first):
        k = pl.ds(pl.multiple_of((me.t + rank) % 4 * cols, cols), cols)

        def one(m, _):
            r = pl.ds(pl.multiple_of(m * part, part), part)
            lhs = rows[b, r]
            g, u = dot(lhs, wg[k, :]), dot(lhs, wu[k, :])
            if first:
                gacc[r] = g
                uacc[r] = u
            else:
                gacc[r] += g
                uacc[r] += u
            return 0

        lax.fori_loop(0, n_all // part, one, 0)

    up_gate(0, 0, True)
    up_gate(1, 3, False)
    up_gate(2, 1, False)

    def last_pair(p, _):
        await_bytes(arr.at[3, 2 * p], xr_sem.at[2, 2 * p])
        await_bytes(arr.at[3, 2 * p + 1], xr_sem.at[2, 2 * p + 1])
        unpack(3, p)
        return 0

    lax.fori_loop(0, n_z // 2, last_pair, 0)
    k3 = pl.ds(pl.multiple_of((me.t + 2) % 4 * cols, cols), cols)

    def act(m, _):
        r = pl.ds(pl.multiple_of(m * part, part), part)
        lhs = rows[3, r]
        g = gacc[r] + dot(lhs, wg[k3, :])
        u = uacc[r] + dot(lhs, wu[k3, :])
        hid[r] = (g / (1.0 + jnp.exp(-g)) * u).astype(BF)
        return 0

    lax.fori_loop(0, n_all // part, act, 0)
    loads[2].wait()

    def down(q, rank):
        return dot(hid[q * part : (q + 1) * part], wd[:, pl.ds(pl.multiple_of((me.t + rank) % 4 * cols, cols), cols)])

    def send_far(q):
        far[q] = down(q, 2).astype(BF)
        remote(far.at[q], relay.at[q], rs_send.at[0, q], relay_sem.at[q], me.x(1 if q < 2 else 3)).start()

    def send_side(q, right, add):
        buf, dst, sem, rank = (to_r, from_l, fl_sem, 1) if right else (to_l, from_r, fr_sem, 3)
        y = down(q, rank)
        if add:
            await_bytes(relay.at[q], relay_sem.at[q])
            y = y + relay[q].astype(F32)
        buf[q] = y.astype(BF)
        remote(buf.at[q], dst.at[q], rs_send.at[1 if right else 2, q], sem.at[q], me.x(1 if right else 3)).start()

    def finish(q):
        y = down(q, 0)
        await_bytes(from_l.at[q], fl_sem.at[q])
        await_bytes(from_r.at[q], fr_sem.at[q])
        y = (y + from_l[q].astype(F32) + from_r[q].astype(F32)).astype(BF)
        ext = dot(pk_extra[...], y[:, 3 * 128 :])
        packed = dot(pk_main[...], y[:, : 3 * 128]) + jnp.concatenate([ext[256 * j : 256 * (j + 1)] for j in range(3)], axis=1)
        retb[2 * q : 2 * q + 2] = packed.astype(BF).reshape(2, SRC, MSG, 3 * 128)
        mine_e = me.z * SRC + me.s8
        for o in (2 * q, 2 * q + 1):
            z = (me.z - me.row(o) + n_z) % n_z

            def send(i, _):
                s = (me.s8 + i) % SRC
                remote(retb.at[o, s], reti.at[mine_e], ret_send, ret_sem, me.at(z, s)).start()
                return 0

            lax.fori_loop(1 if o == 0 else 0, SRC, send, 0)
        if q == 0:
            pltpu.make_async_copy(retb.at[0, me.s8], reti.at[mine_e], ret_sem).start()

    for first in (0, 1):
        send_far(first)
        send_far(first + 2)
        send_side(first + 2, True, False)
        send_side(first, False, False)
        send_side(first, True, True)
        send_side(first + 2, False, True)
    for q in (0, 2, 1, 3):
        finish(q)

    await_bytes(reti, ret_sem)
    res = reti[...].reshape(64 * MSG, 3 * 128)
    mixed = dot(wmix[0, 0], res) + dot(wmix[0, 1], res)
    last = jnp.zeros((n_rows, 128), F32)
    for j in range(3):
        piece = res[:, 128 * j : 128 * (j + 1)]
        last = last + dot(wmix[1 + j, 0], piece) + dot(wmix[1 + j, 1], piece)
    fino[:, :, : 3 * 128] = mixed.astype(BF).reshape(4, quarter, 3 * 128)
    fino[:, :, 3 * 128 :] = last.astype(BF).reshape(4, quarter, 128)
    for step in (1, 2, 3):
        remote(fino.at[(me.t + step) % 4], fini.at[step - 1], fin_send.at[step - 1], fin_sem.at[step - 1], me.x(step)).start()
    out[:, mine] = fino[me.t]
    for step in (1, 2, 3):
        await_bytes(fini.at[step - 1], fin_sem.at[step - 1])
        theirs = pl.ds(pl.multiple_of((me.t + 4 - step) % 4 * cols, cols), cols)
        out[:, theirs] = fini[step - 1]

    for step in (0, 1, 2):
        await_bytes(fini.at[step], fin_send.at[step])
    for q in range(4):
        for k in range(3):
            await_bytes(far.at[q], rs_send.at[k, q])
    for b, k, n in ((0, 0, n_z), (0, 1, n_z), (1, 0, n_z // 2), (2, 1, n_z // 2)):
        await_bytes(arr.at[b, pl.ds(0, n)], xs_sem.at[b, k])
    for buf, sem in ((outb, out_sem), (retb, ret_send)):
        await_bytes(buf.at[pl.ds(1, n_z - 1)], sem)
        await_bytes(buf.at[0, pl.ds(1, SRC - 1)], sem)


def experts_part(moe_tokens, moe_gain, routes, route_weights, w_gate, w_up, w_down):
    n_z = lax.axis_size("ep_0")
    n_rows, model = moe_tokens.shape
    ff = w_gate.shape[2]
    cols = model // 4
    consts = fixed_selects()
    vm = pl.BlockSpec(memory_space=pltpu.VMEM)
    hbm = pl.BlockSpec(memory_space=pl.ANY)
    chunk = (4, 192, cols)
    dma = pltpu.SemaphoreType.DMA
    slots = n_z * SRC * CAP
    return pl.pallas_call(
        functools.partial(experts_kernel, n_z),
        out_shape=jax.ShapeDtypeStruct((n_rows // 4, model), BF),
        in_specs=[vm] * 9 + [hbm] * 3,
        out_specs=vm,
        scratch_shapes=[
            pltpu.VMEM((model, ff), BF),
            pltpu.VMEM((model, ff), BF),
            pltpu.VMEM((ff, model), BF),
            pltpu.VMEM((n_rows, cols), BF),
            pltpu.VMEM((n_z, SRC, MSG, 384), BF),
            pltpu.VMEM((4, n_z, SRC, MSG, 384), BF),
            pltpu.VMEM((4, slots, cols), BF),
            pltpu.VMEM((slots, ff), F32),
            pltpu.VMEM((slots, ff), F32),
            pltpu.VMEM((slots, ff), BF),
            pltpu.VMEM((4, 2, n_rows, 64 * MSG), BF),
            pltpu.VMEM(chunk, BF),
            pltpu.VMEM(chunk, BF),
            pltpu.VMEM(chunk, BF),
            pltpu.VMEM(chunk, BF),
            pltpu.VMEM(chunk, BF),
            pltpu.VMEM(chunk, BF),
            pltpu.VMEM((n_z, SRC, MSG, 384), BF),
            pltpu.VMEM((n_z * SRC, MSG, 384), BF),
            pltpu.VMEM((4, n_rows // 4, cols), BF),
            pltpu.VMEM((3, n_rows // 4, cols), BF),
            dma((3,)),
            dma((n_z,)),
            dma,
            dma,
            dma((3, 2)),
            dma((3, n_z)),
            dma((3, 4)),
            dma((4,)),
            dma((4,)),
            dma((4,)),
            dma,
            dma,
            dma((3,)),
            dma((3,)),
        ],
        compiler_params=pltpu.CompilerParams(collective_id=1, has_side_effects=True, vmem_limit_bytes=60 * 1024 * 1024),
        name="experts",
    )(
        moe_tokens,
        moe_gain.reshape(1, model),
        routes,
        routes.T,
        route_weights,
        *consts,
        w_gate,
        w_up,
        w_down,
    )


def on_device(
    queries,
    kv_latent,
    rope_key,
    latent_gain,
    w_key_up,
    w_value_up,
    query_gain,
    key_gain,
    rope_gain,
    out_gain,
    moe_tokens,
    moe_gain,
    routes,
    route_weights,
    w_gate,
    w_up,
    w_down,
):
    attended = attention_part(
        queries,
        kv_latent,
        rope_key,
        latent_gain,
        w_key_up,
        w_value_up,
        query_gain,
        key_gain,
        rope_gain,
        out_gain,
    )
    moe_out = experts_part(moe_tokens, moe_gain, routes, route_weights, w_gate, w_up, w_down)
    return (attended, moe_out)


def solution(mesh):
    finer = Mesh(mesh.devices.reshape(8, 4, 2, mesh.shape["tp"]), ("ep_0", "ep_1", "ep_2", "tp"))
    placed = (
        P(EP, "tp"),
        P(EP, None),
        P(EP, None),
        P(),
        P(None, "tp"),
        P(None, "tp"),
        P(),
        P(),
        P(),
        P(),
        P(EP, None),
        P(),
        P(EP, None),
        P(EP, None),
        P(EP, None, "tp"),
        P(EP, None, "tp"),
        P(EP, "tp", None),
    )
    return jax.shard_map(
        on_device,
        mesh=finer,
        in_specs=placed,
        out_specs=(P(EP, "tp"), P(EP_TP, None)),
        check_vma=False,
    )
```

```python
import functools
import math

import jax
import jax.numpy as jnp
import numpy as np
from jax import lax
from jax.experimental import pallas as pl
from jax.experimental.pallas import tpu as pltpu
from jax.sharding import Mesh
from jax.sharding import PartitionSpec as P

BF, F32, I32 = jnp.bfloat16, jnp.float32, jnp.int32
MESH = pl.DeviceIdType.MESH

EP = ("ep_0", "ep_1", "ep_2")
EP_TP = ("ep_0", "ep_1", "ep_2", "tp")


EPS = 1e-06
THETA = 500000.0


def rope_tables(positions, rope_dim):
    freqs = 1.0 / THETA ** (jnp.arange(0, rope_dim, 2, dtype=jnp.float32) / rope_dim)
    angles = positions.astype(jnp.float32)[:, None] * freqs[None, :]
    return (jnp.cos(angles), jnp.sin(angles))


SRC = 8
MSG = 16
CAP = 12


def split_two(v):
    hi = v.astype(BF)
    return hi, (v - hi.astype(F32)).astype(BF)


def fixed_selects():
    packed = np.arange(16 * MSG)
    slot = np.arange(16 * CAP)
    src, s = slot // CAP, slot % CAP
    main = (src * MSG + s)[:, None] == packed[None, :]
    extra = [((src * MSG + CAP + s % 4)[:, None] == packed[None, :]) & (s // 4 == j)[:, None] for j in range(3)]
    unpack_extra = np.concatenate(extra, axis=1)
    pack_extra = np.concatenate([e.T for e in extra], axis=0)
    return [jnp.asarray(a.astype(np.float32), BF) for a in (main, unpack_extra, main.T, pack_extra)]


class Place:
    def __init__(self, n_z):
        self.n_z = n_z
        self.z = lax.axis_index("ep_0")
        self.y = lax.axis_index("ep_1")
        self.c = lax.axis_index("ep_2")
        self.t = lax.axis_index("tp")
        self.s8 = self.y * 2 + self.c

    def row(self, order):
        up = order % 2
        return up * ((order + 1) // 2) + (1 - up) * ((self.n_z - order // 2) % self.n_z)

    def x(self, step):
        return (self.z, self.y, self.c, (self.t + step) % 4)

    def at(self, z, s8):
        return (z, s8 // 2, s8 % 2, self.t)


def greet(pl_, n_z):
    barrier = pltpu.get_barrier_semaphore()

    def one(i, _):
        z, s = (pl_.z + i // SRC) % n_z, (pl_.s8 + i % SRC) % SRC
        pl.semaphore_signal(barrier, inc=1, device_id=pl_.at(z, s), device_id_type=MESH)
        return 0

    lax.fori_loop(1, n_z * SRC, one, 0)
    for step in (1, 2, 3):
        pl.semaphore_signal(barrier, inc=1, device_id=pl_.x(step), device_id_type=MESH)


def met(n_z):
    pl.semaphore_wait(pltpu.get_barrier_semaphore(), n_z * SRC - 1 + 3)


def remote(src, dst, send, recv, device):
    return pltpu.make_async_remote_copy(
        src_ref=src, dst_ref=dst, send_sem=send, recv_sem=recv, device_id=device, device_id_type=MESH
    )


def await_bytes(ref, sem):
    pltpu.make_async_copy(ref, ref, sem).wait()


def dot(a, b):
    return jnp.dot(a, b, preferred_element_type=F32)


def experts_kernel(
    n_z,
    tokens,
    gain,
    routes,
    routes_t,
    weights,
    un_main,
    un_extra,
    pk_main,
    pk_extra,
    wg_hbm,
    wu_hbm,
    wd_hbm,
    out,
    wg,
    wu,
    wd,
    normed,
    outb,
    arr,
    rows,
    gacc,
    uacc,
    hid,
    wmix,
    far,
    to_r,
    to_l,
    relay,
    from_l,
    from_r,
    retb,
    reti,
    fino,
    fini,
    w_sem,
    own_sem,
    out_sem,
    self_sem,
    xs_sem,
    xr_sem,
    rs_send,
    relay_sem,
    fl_sem,
    fr_sem,
    ret_send,
    ret_sem,
    fin_send,
    fin_sem,
):
    me = Place(n_z)
    greet(me, n_z)
    loads = [
        pltpu.make_async_copy(h.at[0], v, w_sem.at[k]) for k, (h, v) in enumerate(((wg_hbm, wg), (wu_hbm, wu), (wd_hbm, wd)))
    ]
    for load in loads:
        load.start()
    n_rows, model = tokens.shape
    cols = model // 4
    quarter = n_rows // 4

    exp_ids = lax.broadcasted_iota(I32, (64, n_rows), 0)
    ra, rb = routes_t[0:1, :], routes_t[1:2, :]
    hit_a, hit_b = exp_ids == ra, exp_ids == rb
    both = jnp.where(hit_a | hit_b, 1.0, 0.0).astype(BF)
    i0 = lax.broadcasted_iota(I32, (n_rows, n_rows), 0)
    i1 = lax.broadcasted_iota(I32, (n_rows, n_rows), 1)
    same = (i0 // quarter) == (i1 // quarter)
    earlier_t = jnp.where((i0 < i1) & same, 1.0, 0.0).astype(BF)
    count_t = dot(both, earlier_t)
    base_t = lax.broadcasted_iota(I32, (1, n_rows), 1) // quarter * 3

    def places(hit, chosen):
        s = base_t + jnp.sum(jnp.where(hit, count_t, 0.0), axis=0, keepdims=True).astype(I32)
        return chosen * MSG + s, chosen * MSG + CAP + s % 4 + 2048 * (s // 4)

    (ma, xa), (mb, xb) = places(hit_a, ra), places(hit_b, rb)

    v = tokens[...].astype(F32)
    scale = lax.rsqrt(jnp.mean(v * v, axis=-1, keepdims=True) + EPS)
    mine = pl.ds(pl.multiple_of(me.t * cols, cols), cols)
    normed[...] = (tokens[:, mine].astype(F32) * scale * gain[:, mine]).astype(BF)

    met(n_z)

    def dispatch(o, _):
        z = (me.z + me.row(o)) % n_z
        first = z * SRC * MSG
        ids = lax.broadcasted_iota(I32, (SRC * MSG, n_rows), 0) + first
        main = jnp.where((ids == ma) | (ids == mb), 1.0, 0.0).astype(BF)
        block = dot(main, normed[:, : 3 * 128])
        extra = []
        for j in range(3):
            idj = ids + 2048 * j
            sel = jnp.where((idj == xa) | (idj == xb), 1.0, 0.0).astype(BF)
            extra.append(dot(sel, normed[:, 3 * 128 :]))
        block = block + jnp.concatenate(extra, axis=1)
        outb[o] = block.astype(BF).reshape(SRC, MSG, 3 * 128)

        def send(i, _):
            s = (me.s8 + i) % SRC
            remote(outb.at[o, s], arr.at[0, o, me.s8], out_sem, own_sem.at[o], me.at(z, s)).start()
            return 0

        lax.fori_loop(jnp.where(o == 0, 1, 0), SRC, send, 0)
        return 0

    lax.fori_loop(0, n_z, dispatch, 0)
    pltpu.make_async_copy(outb.at[0, me.s8], arr.at[0, 0, me.s8], own_sem.at[0]).start()

    lane_e = lax.broadcasted_iota(I32, (n_rows, 128), 1)
    ca, cb = routes[:, 0:1], routes[:, 1:2]
    on_a, on_b = lane_e == ca, lane_e == cb
    earlier = jnp.where((i1 < i0) & same, 1.0, 0.0).astype(BF)
    count = dot(earlier, jnp.where(on_a | on_b, 1.0, 0.0).astype(BF))
    base = lax.broadcasted_iota(I32, (n_rows, 1), 0) // quarter * 3
    wa, wb = weights[:, 0:1], weights[:, 1:2]

    def places_c(hit, chosen):
        s = base + jnp.sum(jnp.where(hit, count, 0.0), axis=1, keepdims=True).astype(I32)
        return chosen * MSG + s, chosen * MSG + CAP + s % 4 + 2048 * (s // 4)

    (cma, cxa), (cmb, cxb) = places_c(on_a, ca), places_c(on_b, cb)

    def mix(k, _):
        lanes = lax.broadcasted_iota(I32, (n_rows, 64 * MSG), 1)
        idk = lanes + 2048 * (k - 1)
        pa, pb = jnp.where(k == 0, cma - 2048, cxa), jnp.where(k == 0, cmb - 2048, cxb)
        w = jnp.where(idk == pa, wa, 0.0) + jnp.where(idk == pb, wb, 0.0)
        hi, lo = split_two(w)
        wmix[k, 0] = hi
        wmix[k, 1] = lo
        return 0

    lax.fori_loop(0, 4, mix, 0)

    def pass_on(b, o, step, dst):
        remote(arr.at[b, o], arr.at[dst, o], xs_sem.at[b, step % 4 // 2], xr_sem.at[dst - 1, o], me.x(step)).start()

    def unpack(b, p):
        packed = arr[b, pl.ds(2 * p, 2)].reshape(2 * SRC * MSG, 3 * 128)
        tiles = jnp.concatenate([packed[:, 128 * j : 128 * (j + 1)] for j in range(3)], axis=0)
        r = pl.ds(pl.multiple_of(p * 192, 192), 192)
        rows[b, r, : 3 * 128] = dot(un_main[...], packed).astype(BF)
        rows[b, r, 3 * 128 :] = dot(un_extra[...], tiles).astype(BF)

    def gather(o, _):
        await_bytes(arr.at[0, o], own_sem.at[o])
        pass_on(0, o, 1, 1)
        pass_on(0, o, 3, 2)

        @pl.when(o % 2 == 1)
        def _():
            unpack(0, o // 2)

        return 0

    def relay_on(o):
        await_bytes(arr.at[1, o], xr_sem.at[0, o])
        await_bytes(arr.at[2, o], xr_sem.at[1, o])

        @pl.when(o % 2 == 0)
        def _():
            pass_on(1, o, 1, 3)

        @pl.when(o % 2 == 1)
        def _():
            pass_on(2, o, 3, 3)
            unpack(1, o // 2)
            unpack(2, o // 2)

    def gather_step(o, _):
        gather(o, 0)
        relay_on(o - 1)
        return 0

    gather(0, 0)
    lax.fori_loop(1, n_z, gather_step, 0)
    relay_on(n_z - 1)

    loads[0].wait()
    loads[1].wait()
    n_all = rows.shape[1]
    part = 192
    sides = ((0, 0), (1, 3), (2, 1), (3, 2))

    def up_gate(b, rank, first):
        k = pl.ds(pl.multiple_of((me.t + rank) % 4 * cols, cols), cols)

        def one(m, _):
            r = pl.ds(pl.multiple_of(m * part, part), part)
            lhs = rows[b, r]
            g, u = dot(lhs, wg[k, :]), dot(lhs, wu[k, :])
            if first:
                gacc[r] = g
                uacc[r] = u
            else:
                gacc[r] += g
                uacc[r] += u
            return 0

        lax.fori_loop(0, n_all // part, one, 0)

    up_gate(0, 0, True)
    up_gate(1, 3, False)
    up_gate(2, 1, False)

    def last_pair(p, _):
        await_bytes(arr.at[3, 2 * p], xr_sem.at[2, 2 * p])
        await_bytes(arr.at[3, 2 * p + 1], xr_sem.at[2, 2 * p + 1])
        unpack(3, p)
        return 0

    lax.fori_loop(0, n_z // 2, last_pair, 0)
    k3 = pl.ds(pl.multiple_of((me.t + 2) % 4 * cols, cols), cols)

    def act(m, _):
        r = pl.ds(pl.multiple_of(m * part, part), part)
        lhs = rows[3, r]
        g = gacc[r] + dot(lhs, wg[k3, :])
        u = uacc[r] + dot(lhs, wu[k3, :])
        hid[r] = (g / (1.0 + jnp.exp(-g)) * u).astype(BF)
        return 0

    lax.fori_loop(0, n_all // part, act, 0)
    loads[2].wait()

    def down(q, rank):
        return dot(hid[q * part : (q + 1) * part], wd[:, pl.ds(pl.multiple_of((me.t + rank) % 4 * cols, cols), cols)])

    def send_far(q):
        far[q] = down(q, 2).astype(BF)
        remote(far.at[q], relay.at[q], rs_send.at[0, q], relay_sem.at[q], me.x(1 if q < 2 else 3)).start()

    def send_side(q, right, add):
        buf, dst, sem, rank = (to_r, from_l, fl_sem, 1) if right else (to_l, from_r, fr_sem, 3)
        y = down(q, rank)
        if add:
            await_bytes(relay.at[q], relay_sem.at[q])
            y = y + relay[q].astype(F32)
        buf[q] = y.astype(BF)
        remote(buf.at[q], dst.at[q], rs_send.at[1 if right else 2, q], sem.at[q], me.x(1 if right else 3)).start()

    def finish(q):
        y = down(q, 0)
        await_bytes(from_l.at[q], fl_sem.at[q])
        await_bytes(from_r.at[q], fr_sem.at[q])
        y = (y + from_l[q].astype(F32) + from_r[q].astype(F32)).astype(BF)
        ext = dot(pk_extra[...], y[:, 3 * 128 :])
        packed = dot(pk_main[...], y[:, : 3 * 128]) + jnp.concatenate([ext[256 * j : 256 * (j + 1)] for j in range(3)], axis=1)
        retb[2 * q : 2 * q + 2] = packed.astype(BF).reshape(2, SRC, MSG, 3 * 128)
        mine_e = me.z * SRC + me.s8
        for o in (2 * q, 2 * q + 1):
            z = (me.z - me.row(o) + n_z) % n_z

            def send(i, _):
                s = (me.s8 + i) % SRC
                remote(retb.at[o, s], reti.at[mine_e], ret_send, ret_sem, me.at(z, s)).start()
                return 0

            lax.fori_loop(1 if o == 0 else 0, SRC, send, 0)
        if q == 0:
            pltpu.make_async_copy(retb.at[0, me.s8], reti.at[mine_e], ret_sem).start()

    for first in (0, 1):
        send_far(first)
        send_far(first + 2)
        send_side(first + 2, True, False)
        send_side(first, False, False)
        send_side(first, True, True)
        send_side(first + 2, False, True)
    for q in (0, 2, 1, 3):
        finish(q)

    await_bytes(reti, ret_sem)
    res = reti[...].reshape(64 * MSG, 3 * 128)
    mixed = dot(wmix[0, 0], res) + dot(wmix[0, 1], res)
    last = jnp.zeros((n_rows, 128), F32)
    for j in range(3):
        piece = res[:, 128 * j : 128 * (j + 1)]
        last = last + dot(wmix[1 + j, 0], piece) + dot(wmix[1 + j, 1], piece)
    fino[:, :, : 3 * 128] = mixed.astype(BF).reshape(4, quarter, 3 * 128)
    fino[:, :, 3 * 128 :] = last.astype(BF).reshape(4, quarter, 128)
    for step in (1, 2, 3):
        remote(fino.at[(me.t + step) % 4], fini.at[step - 1], fin_send.at[step - 1], fin_sem.at[step - 1], me.x(step)).start()
    out[:, mine] = fino[me.t]
    for step in (1, 2, 3):
        await_bytes(fini.at[step - 1], fin_sem.at[step - 1])
        theirs = pl.ds(pl.multiple_of((me.t + 4 - step) % 4 * cols, cols), cols)
        out[:, theirs] = fini[step - 1]

    for step in (0, 1, 2):
        await_bytes(fini.at[step], fin_send.at[step])
    for q in range(4):
        for k in range(3):
            await_bytes(far.at[q], rs_send.at[k, q])
    for b, k, n in ((0, 0, n_z), (0, 1, n_z), (1, 0, n_z // 2), (2, 1, n_z // 2)):
        await_bytes(arr.at[b, pl.ds(0, n)], xs_sem.at[b, k])
    for buf, sem in ((outb, out_sem), (retb, ret_send)):
        await_bytes(buf.at[pl.ds(1, n_z - 1)], sem)
        await_bytes(buf.at[0, pl.ds(1, SRC - 1)], sem)


def experts_part(moe_tokens, moe_gain, routes, route_weights, w_gate, w_up, w_down):
    n_z = lax.axis_size("ep_0")
    n_rows, model = moe_tokens.shape
    ff = w_gate.shape[2]
    cols = model // 4
    consts = fixed_selects()
    vm = pl.BlockSpec(memory_space=pltpu.VMEM)
    hbm = pl.BlockSpec(memory_space=pl.ANY)
    chunk = (4, 192, cols)
    dma = pltpu.SemaphoreType.DMA
    slots = n_z * SRC * CAP
    return pl.pallas_call(
        functools.partial(experts_kernel, n_z),
        out_shape=jax.ShapeDtypeStruct((n_rows // 4, model), BF),
        in_specs=[vm] * 9 + [hbm] * 3,
        out_specs=vm,
        scratch_shapes=[
            pltpu.VMEM((model, ff), BF),
            pltpu.VMEM((model, ff), BF),
            pltpu.VMEM((ff, model), BF),
            pltpu.VMEM((n_rows, cols), BF),
            pltpu.VMEM((n_z, SRC, MSG, 384), BF),
            pltpu.VMEM((4, n_z, SRC, MSG, 384), BF),
            pltpu.VMEM((4, slots, cols), BF),
            pltpu.VMEM((slots, ff), F32),
            pltpu.VMEM((slots, ff), F32),
            pltpu.VMEM((slots, ff), BF),
            pltpu.VMEM((4, 2, n_rows, 64 * MSG), BF),
            pltpu.VMEM(chunk, BF),
            pltpu.VMEM(chunk, BF),
            pltpu.VMEM(chunk, BF),
            pltpu.VMEM(chunk, BF),
            pltpu.VMEM(chunk, BF),
            pltpu.VMEM(chunk, BF),
            pltpu.VMEM((n_z, SRC, MSG, 384), BF),
            pltpu.VMEM((n_z * SRC, MSG, 384), BF),
            pltpu.VMEM((4, n_rows // 4, cols), BF),
            pltpu.VMEM((3, n_rows // 4, cols), BF),
            dma((3,)),
            dma((n_z,)),
            dma,
            dma,
            dma((3, 2)),
            dma((3, n_z)),
            dma((3, 4)),
            dma((4,)),
            dma((4,)),
            dma((4,)),
            dma,
            dma,
            dma((3,)),
            dma((3,)),
        ],
        compiler_params=pltpu.CompilerParams(collective_id=1, has_side_effects=True, vmem_limit_bytes=60 * 1024 * 1024),
        name="experts",
    )(
        moe_tokens,
        moe_gain.reshape(1, model),
        routes,
        routes.T,
        route_weights,
        *consts,
        w_gate,
        w_up,
        w_down,
    )


HEAD = 128
ROPE = 64
UP, DOWN = 4, 3


class Attention:
    def __init__(self, n_z, me, ins, out, buf, sem):
        self.n_z, self.me, self.ins, self.out, self.buf, self.sem = n_z, me, ins, out, buf, sem

    def prepare(self):
        me = self.me
        (queries, kv_latent, rope2, lat_gain, wk, wv, qn_gain, qr_gain, key_gain, rope_gain, _, cos2, sin2) = self.ins
        kv, rk, kvb, rkb, q_all, qb = (self.buf[k] for k in ("kv", "rk", "kvb", "rkb", "q_all", "qb"))
        n = queries.shape[0]
        lane = lax.broadcasted_iota(I32, (n, 128), 1)
        low = lane < ROPE

        def turned(v):
            other = jnp.where(lane % ROPE < ROPE // 2, pltpu.roll(v, 128 - ROPE // 2, 1), pltpu.roll(v, ROPE // 2, 1))
            return v * cos2[...] + other * sin2[...]

        v = kv_latent[...].astype(F32)
        latent = (v * lax.rsqrt(jnp.mean(v * v, axis=-1, keepdims=True) + EPS) * lat_gain[...]).astype(BF)
        keys = dot(latent, wk[...])
        vals = dot(latent, wv[...]).astype(BF)
        for h in (0, 1):
            k = keys[:, HEAD * h : HEAD * (h + 1)]
            k = k * lax.rsqrt(jnp.mean(k * k, axis=-1, keepdims=True) + EPS) * key_gain[...]
            kvb[h, :, :HEAD] = k.astype(BF)
            kvb[h, :, HEAD:] = vals[:, HEAD * h : HEAD * (h + 1)]
        r = rope2[...].astype(F32)
        r = turned(r * lax.rsqrt(jnp.mean(r * r, axis=-1, keepdims=True) + EPS) * rope_gain[...])
        rkb[...] = jnp.where(low[: n // 2], r[: n // 2], r[n // 2 :]).astype(BF)

        t0, t1, t2 = (queries[:, 128 * j : 128 * (j + 1)].astype(F32) for j in range(3))
        total = lambda a: jnp.sum(a, axis=-1, keepdims=True)
        s1 = t1 * t1
        width = HEAD + ROPE
        inv0 = lax.rsqrt((total(t0 * t0) + total(jnp.where(low, s1, 0.0))) / width + EPS)
        inv1 = lax.rsqrt((total(t2 * t2) + total(jnp.where(low, 0.0, s1))) / width + EPS)
        nope1 = jnp.where(low, pltpu.roll(t1, ROPE, 1), pltpu.roll(t2, ROPE, 1))
        turn = turned(jnp.where(low, t1 * inv0, t2 * inv1) * qr_gain[...])
        qb[0, :, :HEAD] = (t0 * inv0 * qn_gain[...]).astype(BF)
        qb[1, :, :HEAD] = (nope1 * inv1 * qn_gain[...]).astype(BF)
        qb[0, :, HEAD:] = jnp.where(low, turn, 0.0).astype(BF)
        qb[1, :, HEAD:] = jnp.where(low, 0.0, turn).astype(BF)
        q_all[me.s8] = qb[me.c]
        kv[0, self.mine(256)] = kvb[me.c]
        rk[0, self.mine(128)] = rkb[...]

    def mine(self, n):
        return pl.ds(pl.multiple_of(self.me.c * n, n), n)

    def send_first(self):
        me, b, s = self.me, self.buf, self.sem
        other = (me.z, me.y, 1 - me.c, me.t)
        remote(b["kvb"].at[1 - me.c], b["kv"].at[0, self.mine(256)], s["kv_out"].at[0], s["kv_in"].at[0], other).start()
        remote(b["rkb"], b["rk"].at[0, self.mine(128)], s["kv_out"].at[1], s["rk_in"].at[0], other).start()

        def one(i, _):
            d = (me.s8 + i) % SRC
            remote(b["qb"].at[d % 2], b["q_all"].at[me.s8], s["q_out"], s["q_in"], me.at(me.z, d)).start()
            return 0

        lax.fori_loop(1, SRC, one, 0)

    def first_in(self):
        b, s = self.buf, self.sem
        await_bytes(b["kvb"].at[0], s["kv_in"].at[0])
        await_bytes(b["rkb"], s["rk_in"].at[0])

    def queries_in(self):
        await_bytes(self.buf["q_all"].at[pl.ds(0, SRC - 1)], self.sem["q_in"])

    def has(self, slot):
        z = self.me.z
        if slot <= UP:
            return z >= slot
        return (z + slot - UP) % self.n_z < DOWN

    def uses(self, slot):
        z = self.me.z
        return z >= slot if slot <= UP else z + slot - UP >= self.n_z

    def sends(self, slot, up):
        z = self.me.z
        if up:
            return (z <= self.n_z - 2) & (z >= slot)
        back = 0 if slot == 0 else slot - UP
        return (z + back) % self.n_z < DOWN

    def _copies(self, slot, up):
        me, b, s = self.me, self.buf, self.sem
        to = slot + 1 if up else (UP + 1 if slot == 0 else slot + 1)
        z = (me.z + (1 if up else self.n_z - 1)) % self.n_z
        where = (z, me.y, me.c, me.t)
        return (
            remote(b["kv"].at[slot], b["kv"].at[to], s["hop_out"].at[to, 0], s["kv_in"].at[to], where),
            remote(b["rk"].at[slot], b["rk"].at[to], s["hop_out"].at[to, 1], s["rk_in"].at[to], where),
        )

    def hop(self, slot, up):
        @pl.when(self.sends(slot, up))
        def _():
            for copy in self._copies(slot, up):
                copy.start()

    def arrive(self, slot):
        b, s = self.buf, self.sem

        @pl.when(self.has(slot))
        def _():
            await_bytes(b["kv"].at[slot], s["kv_in"].at[slot])
            await_bytes(b["rk"].at[slot], s["rk_in"].at[slot])

        if slot < UP:
            self.hop(slot, True)
        elif UP < slot < UP + DOWN:
            self.hop(slot, False)

    def attend(self, slot):
        @pl.when(self.uses(slot))
        def _():
            self._attend(slot)

    def _attend(self, slot):
        me = self.me
        kv, rk, q_all, acc, kop, vop = (self.buf[k] for k in ("kv", "rk", "q_all", "acc", "kop", "vop"))
        n_keys = kv.shape[1]
        packed = rk[slot].astype(F32)
        rolled = pltpu.roll(packed, ROPE, 1)
        low = lax.broadcasted_iota(I32, packed.shape, 1) < ROPE
        lo = jnp.where(low, packed, rolled).astype(BF)
        hi = jnp.where(low, rolled, packed).astype(BF)
        kop[:, :HEAD] = kv[slot, :, :HEAD]
        for half in (0, 1):
            kop[256 * half : 256 * half + 128, HEAD:] = lo[128 * half : 128 * half + 128]
            kop[256 * half + 128 : 256 * half + 256, HEAD:] = hi[128 * half : 128 * half + 128]
        vop[:, :HEAD] = kv[slot, :, HEAD:]
        scale = (HEAD + ROPE) ** (-0.5) * math.log2(math.e)
        per = 512

        def one(m, _):
            q = q_all[pl.ds(2 * m, 2)].reshape(per, 2 * HEAD)
            s = lax.dot_general(q, kop[...], (((1,), (1,)), ((), ())), preferred_element_type=F32)
            e = jnp.exp2(s * scale)
            if slot == 0:
                at_q = lax.broadcasted_iota(I32, (per, n_keys), 0) + m * per
                at_k = lax.broadcasted_iota(I32, (per, n_keys), 1) + me.y * n_keys
                e = jnp.where(at_q >= at_k, e, 0.0)
            got = dot(e.astype(BF), vop[...]).reshape(2, 256, 2 * HEAD)
            if slot == 0:
                acc[pl.ds(2 * m, 2)] = got
            else:
                acc[pl.ds(2 * m, 2)] += got
            return 0

        lax.fori_loop(0, SRC * 256 // per, one, 0)

    def ones(self):
        vop = self.buf["vop"]
        vop[:, HEAD:] = jnp.ones((vop.shape[0], HEAD), BF)

    def send_sums(self):
        me, b, s = self.me, self.buf, self.sem
        acc, ob, db, od, dd = (b[k] for k in ("acc", "ob", "db", "od", "dd"))

        def halves(m):
            a = acc[m]
            return a[:, :HEAD].astype(BF), jnp.transpose(a[:, HEAD:])[:8]

        def one(i, _):
            m = (me.s8 + i) % SRC
            ob[m], db[m] = halves(m)
            where = me.at(me.z, m)
            remote(ob.at[m], od.at[me.s8], s["o_out"].at[0], s["o_in"].at[0], where).start()
            remote(db.at[m], dd.at[me.s8], s["o_out"].at[1], s["o_in"].at[1], where).start()
            return 0

        lax.fori_loop(1, SRC, one, 0)
        od[me.s8], dd[me.s8] = halves(me.s8)

    def finish(self):
        b, s = self.buf, self.sem
        od, dd = b["od"], b["dd"]
        out_gain = self.ins[10]
        await_bytes(od.at[pl.ds(0, SRC - 1)], s["o_in"].at[0])
        await_bytes(dd.at[pl.ds(0, SRC - 1)], s["o_in"].at[1])
        for h in (0, 1):
            o = sum(od[2 * y + h].astype(F32) for y in range(4))
            d = sum(dd[2 * y + h] for y in range(4))
            den = jnp.transpose(jnp.broadcast_to(d[0:1], (HEAD, d.shape[1])))
            m = o / den
            m = m * lax.rsqrt(jnp.mean(m * m, axis=-1, keepdims=True) + EPS) * out_gain[...]
            self.out[:, HEAD * h : HEAD * (h + 1)] = m.astype(BF)

    def drain(self):
        b, s = self.buf, self.sem
        await_bytes(b["kvb"].at[0], s["kv_out"].at[0])
        await_bytes(b["rkb"], s["kv_out"].at[1])
        await_bytes(b["q_all"].at[pl.ds(0, SRC - 1)], s["q_out"])
        for slot, up in [(k, True) for k in range(UP)] + [(0, False)] + [(UP + k, False) for k in range(1, DOWN)]:

            @pl.when(self.sends(slot, up))
            def _():
                for copy in self._copies(slot, up):
                    copy.wait_send()

        await_bytes(b["od"].at[pl.ds(0, SRC - 1)], s["o_out"].at[0])
        await_bytes(b["dd"].at[pl.ds(0, SRC - 1)], s["o_out"].at[1])


ATT_BUFS = {
    "kv": ((8, 512, 256), "bf"),
    "rk": ((8, 256, 128), "bf"),
    "kvb": ((2, 256, 256), "bf"),
    "rkb": ((128, 128), "bf"),
    "q_all": ((8, 256, 256), "bf"),
    "qb": ((2, 256, 256), "bf"),
    "acc": ((8, 256, 256), "f"),
    "kop": ((512, 256), "bf"),
    "vop": ((512, 256), "bf"),
    "ob": ((8, 256, 128), "bf"),
    "db": ((8, 8, 256), "f"),
    "od": ((8, 256, 128), "bf"),
    "dd": ((8, 8, 256), "f"),
}
ATT_SEMS = {"kv_out": (2,), "kv_in": (8,), "rk_in": (8,), "q_out": None, "q_in": None, "hop_out": (8, 2), "o_out": (2,), "o_in": (2,)}


def att_scratch():
    bufs = [pltpu.VMEM(shape, BF if kind == "bf" else F32) for shape, kind in ATT_BUFS.values()]
    sems = [pltpu.SemaphoreType.DMA if n is None else pltpu.SemaphoreType.DMA(n) for n in ATT_SEMS.values()]
    return bufs + sems


def att_refs(refs):
    n = len(ATT_BUFS)
    return dict(zip(ATT_BUFS, refs[:n])), dict(zip(ATT_SEMS, refs[n:]))


def att_inputs(queries, kv_latent, rope_key, latent_gain, w_key_up, w_value_up, query_gain, key_gain, rope_gain, out_gain):
    n = queries.shape[0]
    positions = lax.axis_index(EP) * n + jnp.arange(n, dtype=I32)
    cos, sin = rope_tables(positions, ROPE)
    row = lambda g: g.reshape(1, -1)
    twice = lambda g: jnp.concatenate([g, g], axis=-1)
    return (
        queries,
        kv_latent,
        twice(rope_key),
        row(latent_gain),
        w_key_up,
        w_value_up,
        row(query_gain[:HEAD]),
        row(twice(query_gain[HEAD:])),
        row(key_gain),
        row(twice(rope_gain)),
        row(out_gain),
        twice(twice(cos)),
        twice(jnp.concatenate([-sin, sin], axis=-1)),
    )


def attention_kernel(n_z, *refs):
    ins, out, rest = refs[:13], refs[13], refs[14:]
    me = Place(n_z)
    buf, sem = att_refs(rest)
    barrier = pltpu.get_barrier_semaphore()

    def one(i, _):
        pl.semaphore_signal(barrier, inc=1, device_id=me.at(me.z, (me.s8 + i) % SRC), device_id_type=MESH)
        return 0

    lax.fori_loop(1, SRC, one, 0)
    for step in (1, n_z - 1):
        pl.semaphore_signal(barrier, inc=1, device_id=((me.z + step) % n_z, me.y, me.c, me.t), device_id_type=MESH)
    att = Attention(n_z, me, ins, out, buf, sem)
    att.prepare()
    att.ones()
    pl.semaphore_wait(barrier, SRC - 1 + 2)
    att.send_first()
    att.first_in()
    att.hop(0, True)
    att.hop(0, False)
    att.queries_in()
    att.attend(0)
    for k in range(1, UP + 1):
        att.arrive(k)
        if k <= DOWN:
            att.arrive(UP + k)
        att.attend(k)
        if k <= DOWN:
            att.attend(UP + k)
    att.send_sums()
    att.finish()
    att.drain()


def attention_part(*args):
    n_z = lax.axis_size("ep_0")
    ins = att_inputs(*args)
    vm = pl.BlockSpec(memory_space=pltpu.VMEM)
    return pl.pallas_call(
        functools.partial(attention_kernel, n_z),
        out_shape=jax.ShapeDtypeStruct((256, 256), BF),
        in_specs=[vm] * 13,
        out_specs=vm,
        scratch_shapes=att_scratch(),
        compiler_params=pltpu.CompilerParams(collective_id=2, has_side_effects=True, vmem_limit_bytes=60 * 1024 * 1024),
        name="attention",
    )(*ins)


def on_device(
    queries,
    kv_latent,
    rope_key,
    latent_gain,
    w_key_up,
    w_value_up,
    query_gain,
    key_gain,
    rope_gain,
    out_gain,
    moe_tokens,
    moe_gain,
    routes,
    route_weights,
    w_gate,
    w_up,
    w_down,
):
    attended = attention_part(
        queries,
        kv_latent,
        rope_key,
        latent_gain,
        w_key_up,
        w_value_up,
        query_gain,
        key_gain,
        rope_gain,
        out_gain,
    )
    moe_out = experts_part(moe_tokens, moe_gain, routes, route_weights, w_gate, w_up, w_down)
    return (attended, moe_out)


def solution(mesh):
    finer = Mesh(mesh.devices.reshape(8, 4, 2, mesh.shape["tp"]), ("ep_0", "ep_1", "ep_2", "tp"))
    placed = (
        P(EP, "tp"),
        P(EP, None),
        P(EP, None),
        P(),
        P(None, "tp"),
        P(None, "tp"),
        P(),
        P(),
        P(),
        P(),
        P(EP, None),
        P(),
        P(EP, None),
        P(EP, None),
        P(EP, None, "tp"),
        P(EP, None, "tp"),
        P(EP, "tp", None),
    )
    return jax.shard_map(
        on_device,
        mesh=finer,
        in_specs=placed,
        out_specs=(P(EP, "tp"), P(EP_TP, None)),
        check_vma=False,
    )
```

```python
import functools
import math

import jax
import jax.numpy as jnp
import numpy as np
from jax import lax
from jax.experimental import pallas as pl
from jax.experimental.pallas import tpu as pltpu
from jax.sharding import Mesh
from jax.sharding import PartitionSpec as P

BF, F32, I32 = jnp.bfloat16, jnp.float32, jnp.int32
MESH = pl.DeviceIdType.MESH

EP = ("ep_0", "ep_1", "ep_2")
EP_TP = ("ep_0", "ep_1", "ep_2", "tp")


EPS = 1e-06
THETA = 500000.0


SRC = 8
MSG = 16
CAP = 12


def split_two(v):
    hi = v.astype(BF)
    return hi, (v - hi.astype(F32)).astype(BF)


def fixed_selects():
    packed = np.arange(16 * MSG)
    slot = np.arange(16 * CAP)
    src, s = slot // CAP, slot % CAP
    main = (src * MSG + s)[:, None] == packed[None, :]
    extra = [((src * MSG + CAP + s % 4)[:, None] == packed[None, :]) & (s // 4 == j)[:, None] for j in range(3)]
    unpack_extra = np.concatenate(extra, axis=1)
    pack_extra = np.concatenate([e.T for e in extra], axis=0)
    return [jnp.asarray(a.astype(np.float32), BF) for a in (main, unpack_extra, main.T, pack_extra)]


class Place:
    def __init__(self, n_z):
        self.n_z = n_z
        self.z = lax.axis_index("ep_0")
        self.y = lax.axis_index("ep_1")
        self.c = lax.axis_index("ep_2")
        self.t = lax.axis_index("tp")
        self.s8 = self.y * 2 + self.c

    def row(self, order):
        up = order % 2
        return up * ((order + 1) // 2) + (1 - up) * ((self.n_z - order // 2) % self.n_z)

    def x(self, step):
        return (self.z, self.y, self.c, (self.t + step) % 4)

    def at(self, z, s8):
        return (z, s8 // 2, s8 % 2, self.t)


def greet(pl_, n_z):
    barrier = pltpu.get_barrier_semaphore()

    def one(i, _):
        z, s = (pl_.z + i // SRC) % n_z, (pl_.s8 + i % SRC) % SRC
        pl.semaphore_signal(barrier, inc=1, device_id=pl_.at(z, s), device_id_type=MESH)
        return 0

    lax.fori_loop(1, n_z * SRC, one, 0)
    for step in (1, 2, 3):
        pl.semaphore_signal(barrier, inc=1, device_id=pl_.x(step), device_id_type=MESH)


def met(n_z):
    pl.semaphore_wait(pltpu.get_barrier_semaphore(), n_z * SRC - 1 + 3)


def remote(src, dst, send, recv, device):
    return pltpu.make_async_remote_copy(
        src_ref=src, dst_ref=dst, send_sem=send, recv_sem=recv, device_id=device, device_id_type=MESH
    )


def await_bytes(ref, sem):
    pltpu.make_async_copy(ref, ref, sem).wait()


def dot(a, b):
    return jnp.dot(a, b, preferred_element_type=F32)


HEAD = 128
ROPE = 64
PIECE = 512
UP, DOWN = 4, 3


class Attention:
    def __init__(self, n_z, me, ins, out, buf, sem):
        self.n_z, self.me, self.ins, self.out, self.buf, self.sem = n_z, me, ins, out, buf, sem

    def prepare(self):
        me = self.me
        (queries, kv_latent, rope_key, lat_gain, wk, wv, q_gain, key_gain, rope_gain, _, near, far) = self.ins
        twice = lambda a: jnp.concatenate([a, a], axis=-1)
        qn_gain, qr_gain = q_gain[:, :HEAD], twice(q_gain[:, HEAD:])
        place = me.z * SRC + me.s8
        far_cos, far_sin = far[0, pl.ds(place, 1)], far[1, pl.ds(place, 1)]
        cos2 = near[0] * far_cos - near[1] * far_sin
        sin2 = near[1] * far_cos + near[0] * far_sin
        kv, rk, kvb, rkb, q_all, qb = (self.buf[k] for k in ("kv", "rk", "kvb", "rkb", "q_all", "qb"))
        n = queries.shape[0]
        lane = lax.broadcasted_iota(I32, (n, 128), 1)
        low = lane < ROPE
        signed = jnp.where(lane % ROPE < ROPE // 2, -sin2, sin2)

        def turned(v):
            other = jnp.where(lane % ROPE < ROPE // 2, pltpu.roll(v, 128 - ROPE // 2, 1), pltpu.roll(v, ROPE // 2, 1))
            return v * cos2 + other * signed

        v = kv_latent[...].astype(F32)
        latent = (v * lax.rsqrt(jnp.mean(v * v, axis=-1, keepdims=True) + EPS) * lat_gain[...]).astype(BF)
        keys = dot(latent, wk[...])
        vals = dot(latent, wv[...]).astype(BF)
        for h in (0, 1):
            k = keys[:, HEAD * h : HEAD * (h + 1)]
            k = k * lax.rsqrt(jnp.mean(k * k, axis=-1, keepdims=True) + EPS) * key_gain[...]
            kvb[h, :, :HEAD] = k.astype(BF)
            kvb[h, :, HEAD:] = vals[:, HEAD * h : HEAD * (h + 1)]
        r = twice(rope_key[...].astype(F32))
        r = turned(r * lax.rsqrt(jnp.mean(r * r, axis=-1, keepdims=True) + EPS) * twice(rope_gain[...]))
        rkb[...] = jnp.where(low[: n // 2], r[: n // 2], r[n // 2 :]).astype(BF)

        t0, t1, t2 = (queries[:, 128 * j : 128 * (j + 1)].astype(F32) for j in range(3))
        total = lambda a: jnp.sum(a, axis=-1, keepdims=True)
        s1 = t1 * t1
        width = HEAD + ROPE
        inv0 = lax.rsqrt((total(t0 * t0) + total(jnp.where(low, s1, 0.0))) / width + EPS)
        inv1 = lax.rsqrt((total(t2 * t2) + total(jnp.where(low, 0.0, s1))) / width + EPS)
        nope1 = jnp.where(low, pltpu.roll(t1, ROPE, 1), pltpu.roll(t2, ROPE, 1))
        turn = turned(jnp.where(low, t1 * inv0, t2 * inv1) * qr_gain)
        qb[0, :, :HEAD] = (t0 * inv0 * qn_gain).astype(BF)
        qb[1, :, :HEAD] = (nope1 * inv1 * qn_gain).astype(BF)
        qb[0, :, HEAD:] = jnp.where(low, turn, 0.0).astype(BF)
        qb[1, :, HEAD:] = jnp.where(low, 0.0, turn).astype(BF)
        q_all[me.s8] = qb[me.c]
        kv[0, self.mine(256)] = kvb[me.c]
        rk[0, self.mine(128)] = rkb[...]

    def mine(self, n):
        return pl.ds(pl.multiple_of(self.me.c * n, n), n)

    def send_first(self):
        me, b, s = self.me, self.buf, self.sem
        other = (me.z, me.y, 1 - me.c, me.t)
        remote(b["kvb"].at[1 - me.c], b["kv"].at[0, self.mine(256)], s["kv_out"].at[0], s["kv_in"].at[0], other).start()
        remote(b["rkb"], b["rk"].at[0, self.mine(128)], s["kv_out"].at[1], s["rk_in"].at[0], other).start()

        def one(i, _):
            d = (me.s8 + i) % SRC
            remote(b["qb"].at[d % 2], b["q_all"].at[me.s8], s["q_out"], s["q_in"], me.at(me.z, d)).start()
            return 0

        lax.fori_loop(1, SRC, one, 0)

    def first_in(self):
        b, s = self.buf, self.sem
        await_bytes(b["kvb"].at[0], s["kv_in"].at[0])
        await_bytes(b["rkb"], s["rk_in"].at[0])

    def queries_in(self):
        await_bytes(self.buf["q_all"].at[pl.ds(0, SRC - 1)], self.sem["q_in"])

    def has(self, slot):
        z = self.me.z
        if slot <= UP:
            return z >= slot
        return (z + slot - UP) % self.n_z < DOWN

    def uses(self, slot):
        z = self.me.z
        return z >= slot if slot <= UP else z + slot - UP >= self.n_z

    def sends(self, slot, up):
        z = self.me.z
        if up:
            return (z <= self.n_z - 2) & (z >= slot)
        back = 0 if slot == 0 else slot - UP
        return (z + back) % self.n_z < DOWN

    def _copies(self, slot, up):
        me, b, s = self.me, self.buf, self.sem
        to = slot + 1 if up else (UP + 1 if slot == 0 else slot + 1)
        z = (me.z + (1 if up else self.n_z - 1)) % self.n_z
        where = (z, me.y, me.c, me.t)
        return (
            remote(b["kv"].at[slot], b["kv"].at[to], s["hop_out"].at[to, 0], s["kv_in"].at[to], where),
            remote(b["rk"].at[slot], b["rk"].at[to], s["hop_out"].at[to, 1], s["rk_in"].at[to], where),
        )

    def hop(self, slot, up):
        @pl.when(self.sends(slot, up))
        def _():
            for copy in self._copies(slot, up):
                copy.start()

    def arrive(self, slot):
        b, s = self.buf, self.sem

        @pl.when(self.has(slot))
        def _():
            await_bytes(b["kv"].at[slot], s["kv_in"].at[slot])
            await_bytes(b["rk"].at[slot], s["rk_in"].at[slot])

        if slot < UP:
            self.hop(slot, True)
        elif UP < slot < UP + DOWN:
            self.hop(slot, False)

    def attend(self, slot):
        @pl.when(self.uses(slot))
        def _():
            self.load(slot)

            def one(m, _):
                self.piece(slot, m)
                return 0

            lax.fori_loop(0, SRC * 256 // PIECE, one, 0)

    def load(self, slot):
        kv, rk, kop, vop = (self.buf[k] for k in ("kv", "rk", "kop", "vop"))
        packed = rk[slot].astype(F32)
        rolled = pltpu.roll(packed, ROPE, 1)
        low = lax.broadcasted_iota(I32, packed.shape, 1) < ROPE
        lo = jnp.where(low, packed, rolled).astype(BF)
        hi = jnp.where(low, rolled, packed).astype(BF)
        kop[:, :HEAD] = kv[slot, :, :HEAD]
        for half in (0, 1):
            kop[256 * half : 256 * half + 128, HEAD:] = lo[128 * half : 128 * half + 128]
            kop[256 * half + 128 : 256 * half + 256, HEAD:] = hi[128 * half : 128 * half + 128]
        vop[:, :HEAD] = kv[slot, :, HEAD:]

    def piece(self, slot, m):
        q_all, acc, kop, vop = (self.buf[k] for k in ("q_all", "acc", "kop", "vop"))
        n_keys = kop.shape[0]
        scale = (HEAD + ROPE) ** (-0.5) * math.log2(math.e)
        two = pl.ds(2 * m, PIECE // 256)
        q = q_all[two].reshape(PIECE, 2 * HEAD)
        s = lax.dot_general(q, kop[...], (((1,), (1,)), ((), ())), preferred_element_type=F32)
        e = jnp.exp2(s * scale)
        if slot == 0:
            at_q = lax.broadcasted_iota(I32, (PIECE, n_keys), 0) + m * PIECE
            at_k = lax.broadcasted_iota(I32, (PIECE, n_keys), 1) + self.me.y * n_keys
            e = jnp.where(at_q >= at_k, e, 0.0)
        got = dot(e.astype(BF), vop[...]).reshape(PIECE // 256, 256, 2 * HEAD)
        if slot == 0:
            acc[two] = got
        else:
            acc[two] += got

    def ones(self):
        vop = self.buf["vop"]
        vop[:, HEAD:] = jnp.ones((vop.shape[0], HEAD), BF)

    def send_sums(self):
        me, b, s = self.me, self.buf, self.sem
        acc, ob, db, od, dd = (b[k] for k in ("acc", "ob", "db", "od", "dd"))

        def halves(m):
            a = acc[m]
            return a[:, :HEAD].astype(BF), jnp.transpose(a[:, HEAD:])[:8]

        def one(i, _):
            m = (me.s8 + i) % SRC
            ob[m], db[m] = halves(m)
            where = me.at(me.z, m)
            remote(ob.at[m], od.at[me.s8], s["o_out"].at[0], s["o_in"].at[0], where).start()
            remote(db.at[m], dd.at[me.s8], s["o_out"].at[1], s["o_in"].at[1], where).start()
            return 0

        lax.fori_loop(1, SRC, one, 0)
        od[me.s8], dd[me.s8] = halves(me.s8)

    def finish(self):
        b, s = self.buf, self.sem
        od, dd = b["od"], b["dd"]
        out_gain = self.ins[9]
        await_bytes(od.at[pl.ds(0, SRC - 1)], s["o_in"].at[0])
        await_bytes(dd.at[pl.ds(0, SRC - 1)], s["o_in"].at[1])
        for h in (0, 1):
            o = sum(od[2 * y + h].astype(F32) for y in range(4))
            d = sum(dd[2 * y + h] for y in range(4))
            den = jnp.transpose(jnp.broadcast_to(d[0:1], (HEAD, d.shape[1])))
            m = o / den
            m = m * lax.rsqrt(jnp.mean(m * m, axis=-1, keepdims=True) + EPS) * out_gain[...]
            self.out[:, HEAD * h : HEAD * (h + 1)] = m.astype(BF)

    def drain(self):
        b, s = self.buf, self.sem
        await_bytes(b["kvb"].at[0], s["kv_out"].at[0])
        await_bytes(b["rkb"], s["kv_out"].at[1])
        await_bytes(b["q_all"].at[pl.ds(0, SRC - 1)], s["q_out"])
        for slot, up in [(k, True) for k in range(UP)] + [(0, False)] + [(UP + k, False) for k in range(1, DOWN)]:

            @pl.when(self.sends(slot, up))
            def _():
                for copy in self._copies(slot, up):
                    copy.wait_send()

        await_bytes(b["od"].at[pl.ds(0, SRC - 1)], s["o_out"].at[0])
        await_bytes(b["dd"].at[pl.ds(0, SRC - 1)], s["o_out"].at[1])


ATT_BUFS = {
    "kv": ((8, 512, 256), "bf"),
    "rk": ((8, 256, 128), "bf"),
    "kvb": ((2, 256, 256), "bf"),
    "rkb": ((128, 128), "bf"),
    "q_all": ((8, 256, 256), "bf"),
    "qb": ((2, 256, 256), "bf"),
    "acc": ((8, 256, 256), "f"),
    "kop": ((512, 256), "bf"),
    "vop": ((512, 256), "bf"),
    "ob": ((8, 256, 128), "bf"),
    "db": ((8, 8, 256), "f"),
    "od": ((8, 256, 128), "bf"),
    "dd": ((8, 8, 256), "f"),
}
ATT_SEMS = {"kv_out": (2,), "kv_in": (8,), "rk_in": (8,), "q_out": None, "q_in": None, "hop_out": (8, 2), "o_out": (2,), "o_in": (2,)}


def att_scratch():
    bufs = [pltpu.VMEM(shape, BF if kind == "bf" else F32) for shape, kind in ATT_BUFS.values()]
    sems = [pltpu.SemaphoreType.DMA if n is None else pltpu.SemaphoreType.DMA(n) for n in ATT_SEMS.values()]
    return bufs + sems


def att_refs(refs):
    n = len(ATT_BUFS)
    return dict(zip(ATT_BUFS, refs[:n])), dict(zip(ATT_SEMS, refs[n:]))


OWN = (
    "wg",
    "wu",
    "wd",
    "normed",
    "outb",
    "arr",
    "rows",
    "gacc",
    "uacc",
    "hid",
    "wmix",
    "far",
    "to_r",
    "to_l",
    "relay",
    "from_l",
    "from_r",
    "retb",
    "reti",
    "fino",
    "fini",
    "w_sem",
    "own_sem",
    "out_sem",
    "xs_sem",
    "xr_sem",
    "rs_send",
    "relay_sem",
    "fl_sem",
    "fr_sem",
    "ret_send",
    "ret_sem",
    "fin_send",
    "fin_sem",
)


def whole_kernel(n_z, *refs):
    a_in, refs = refs[:12], refs[12:]
    (tokens, gain, routes_t, weights_t, un_main, un_extra, pk_main, pk_extra, wg_hbm, wu_hbm, wd_hbm), refs = refs[:11], refs[11:]
    a_out, out, refs = refs[0], refs[1], refs[2:]
    n_own = len(OWN)
    own = dict(zip(OWN, refs[:n_own]))
    wg, wu, wd, normed, outb, arr = (own[k] for k in ("wg", "wu", "wd", "normed", "outb", "arr"))
    rows, gacc, uacc, hid, wmix, far = (own[k] for k in ("rows", "gacc", "uacc", "hid", "wmix", "far"))
    to_r, to_l, relay, from_l, from_r, retb = (own[k] for k in ("to_r", "to_l", "relay", "from_l", "from_r", "retb"))
    reti, fino, fini, w_sem, own_sem, out_sem = (own[k] for k in ("reti", "fino", "fini", "w_sem", "own_sem", "out_sem"))
    xs_sem, xr_sem, rs_send, relay_sem, fl_sem, fr_sem = (own[k] for k in ("xs_sem", "xr_sem", "rs_send", "relay_sem", "fl_sem", "fr_sem"))
    ret_send, ret_sem, fin_send, fin_sem = (own[k] for k in ("ret_send", "ret_sem", "fin_send", "fin_sem"))
    me = Place(n_z)
    att = Attention(n_z, me, a_in, a_out, *att_refs(refs[n_own:]))
    greet(me, n_z)
    loads = [
        pltpu.make_async_copy(h.at[0], v, w_sem.at[k]) for k, (h, v) in enumerate(((wg_hbm, wg), (wu_hbm, wu), (wd_hbm, wd)))
    ]
    for load in loads:
        load.start()
    n_rows, model = tokens.shape
    cols = model // 4
    quarter = n_rows // 4

    exp_ids = lax.broadcasted_iota(I32, (64, n_rows), 0)
    ra, rb = routes_t[0:1, :], routes_t[1:2, :]
    hit_a, hit_b = exp_ids == ra, exp_ids == rb
    both = jnp.where(hit_a | hit_b, 1.0, 0.0).astype(BF)
    i0 = lax.broadcasted_iota(I32, (n_rows, n_rows), 0)
    i1 = lax.broadcasted_iota(I32, (n_rows, n_rows), 1)
    same = (i0 // quarter) == (i1 // quarter)
    earlier_t = jnp.where((i0 < i1) & same, 1.0, 0.0).astype(BF)
    count_t = dot(both, earlier_t)
    base_t = lax.broadcasted_iota(I32, (1, n_rows), 1) // quarter * 3

    def places(hit, chosen):
        s = base_t + jnp.sum(jnp.where(hit, count_t, 0.0), axis=0, keepdims=True).astype(I32)
        return chosen * MSG + s, chosen * MSG + CAP + s % 4 + 2048 * (s // 4)

    (ma, xa), (mb, xb) = places(hit_a, ra), places(hit_b, rb)

    v = tokens[...].astype(F32)
    scale = lax.rsqrt(jnp.mean(v * v, axis=-1, keepdims=True) + EPS)
    mine = pl.ds(pl.multiple_of(me.t * cols, cols), cols)
    normed[...] = (tokens[:, mine].astype(F32) * scale * gain[:, mine]).astype(BF)

    met(n_z)

    def dispatch(o, _):
        z = (me.z + me.row(o)) % n_z
        first = z * SRC * MSG
        ids = lax.broadcasted_iota(I32, (SRC * MSG, n_rows), 0) + first
        main = jnp.where((ids == ma) | (ids == mb), 1.0, 0.0).astype(BF)
        block = dot(main, normed[:, : 3 * 128])
        extra = []
        for j in range(3):
            idj = ids + 2048 * j
            sel = jnp.where((idj == xa) | (idj == xb), 1.0, 0.0).astype(BF)
            extra.append(dot(sel, normed[:, 3 * 128 :]))
        block = block + jnp.concatenate(extra, axis=1)
        outb[o] = block.astype(BF).reshape(SRC, MSG, 3 * 128)

        def send(i, _):
            s = (me.s8 + i) % SRC
            remote(outb.at[o, s], arr.at[0, o, me.s8], out_sem, own_sem.at[o], me.at(z, s)).start()
            return 0

        lax.fori_loop(jnp.where(o == 0, 1, 0), SRC, send, 0)
        return 0

    lax.fori_loop(0, n_z, dispatch, 0)
    pltpu.make_async_copy(outb.at[0, me.s8], arr.at[0, 0, me.s8], own_sem.at[0]).start()

    att.prepare()
    att.ones()
    att.send_first()

    upright = lambda row: jnp.transpose(jnp.broadcast_to(row, (128, n_rows)))[:, 0:1]
    lane_e = lax.broadcasted_iota(I32, (n_rows, 128), 1)
    ca, cb = (upright(r.astype(F32)).astype(I32) for r in (ra, rb))
    on_a, on_b = lane_e == ca, lane_e == cb
    earlier = jnp.where((i1 < i0) & same, 1.0, 0.0).astype(BF)
    count = dot(earlier, jnp.where(on_a | on_b, 1.0, 0.0).astype(BF))
    base = lax.broadcasted_iota(I32, (n_rows, 1), 0) // quarter * 3
    wa, wb = (upright(weights_t[k : k + 1, :]) for k in (0, 1))

    def places_c(hit, chosen):
        s = base + jnp.sum(jnp.where(hit, count, 0.0), axis=1, keepdims=True).astype(I32)
        return chosen * MSG + s, chosen * MSG + CAP + s % 4 + 2048 * (s // 4)

    (cma, cxa), (cmb, cxb) = places_c(on_a, ca), places_c(on_b, cb)

    def mix(k, _):
        lanes = lax.broadcasted_iota(I32, (n_rows, 64 * MSG), 1)
        idk = lanes + 2048 * (k - 1)
        pa, pb = jnp.where(k == 0, cma - 2048, cxa), jnp.where(k == 0, cmb - 2048, cxb)
        w = jnp.where(idk == pa, wa, 0.0) + jnp.where(idk == pb, wb, 0.0)
        hi, lo = split_two(w)
        wmix[k, 0] = hi
        wmix[k, 1] = lo
        return 0

    lax.fori_loop(0, 4, mix, 0)

    def pass_on(b, o, step, dst):
        remote(arr.at[b, o], arr.at[dst, o], xs_sem.at[b, step % 4 // 2], xr_sem.at[dst - 1, o], me.x(step)).start()

    def unpack(b, p):
        packed = arr[b, pl.ds(2 * p, 2)].reshape(2 * SRC * MSG, 3 * 128)
        tiles = jnp.concatenate([packed[:, 128 * j : 128 * (j + 1)] for j in range(3)], axis=0)
        r = pl.ds(pl.multiple_of(p * 192, 192), 192)
        rows[b, r, : 3 * 128] = dot(un_main[...], packed).astype(BF)
        rows[b, r, 3 * 128 :] = dot(un_extra[...], tiles).astype(BF)

    def gather(o, _):
        await_bytes(arr.at[0, o], own_sem.at[o])
        pass_on(0, o, 1, 1)
        pass_on(0, o, 3, 2)

        @pl.when(o % 2 == 1)
        def _():
            unpack(0, o // 2)

        return 0

    def relay_on(o):
        await_bytes(arr.at[1, o], xr_sem.at[0, o])
        await_bytes(arr.at[2, o], xr_sem.at[1, o])

        @pl.when(o % 2 == 0)
        def _():
            pass_on(1, o, 1, 3)

        @pl.when(o % 2 == 1)
        def _():
            pass_on(2, o, 3, 3)
            unpack(1, o // 2)
            unpack(2, o // 2)

    def gather_step(o, _):
        gather(o, 0)
        relay_on(o - 1)
        return 0

    n_pieces = SRC * 256 // PIECE

    def gather_attend(o, _):
        gather_step(o, 0)
        att.piece(0, o - (n_z - n_pieces))
        return 0

    gather(0, 0)
    lax.fori_loop(1, n_z - n_pieces, gather_step, 0)
    att.first_in()
    att.queries_in()
    att.load(0)
    lax.fori_loop(n_z - n_pieces, n_z, gather_attend, 0)
    att.hop(0, True)
    att.hop(0, False)
    relay_on(n_z - 1)

    loads[0].wait()
    loads[1].wait()
    n_all = rows.shape[1]
    part = 192
    sides = ((0, 0), (1, 3), (2, 1), (3, 2))

    def up_gate(b, rank, first):
        k = pl.ds(pl.multiple_of((me.t + rank) % 4 * cols, cols), cols)

        def one(m, _):
            r = pl.ds(pl.multiple_of(m * part, part), part)
            lhs = rows[b, r]
            g, u = dot(lhs, wg[k, :]), dot(lhs, wu[k, :])
            if first:
                gacc[r] = g
                uacc[r] = u
            else:
                gacc[r] += g
                uacc[r] += u
            return 0

        lax.fori_loop(0, n_all // part, one, 0)

    up_gate(0, 0, True)
    up_gate(1, 3, False)
    up_gate(2, 1, False)

    def last_pair(p, _):
        await_bytes(arr.at[3, 2 * p], xr_sem.at[2, 2 * p])
        await_bytes(arr.at[3, 2 * p + 1], xr_sem.at[2, 2 * p + 1])
        unpack(3, p)
        return 0

    lax.fori_loop(0, n_z // 2, last_pair, 0)
    k3 = pl.ds(pl.multiple_of((me.t + 2) % 4 * cols, cols), cols)

    def act(m, _):
        r = pl.ds(pl.multiple_of(m * part, part), part)
        lhs = rows[3, r]
        g = gacc[r] + dot(lhs, wg[k3, :])
        u = uacc[r] + dot(lhs, wu[k3, :])
        hid[r] = (g / (1.0 + jnp.exp(-g)) * u).astype(BF)
        return 0

    lax.fori_loop(0, n_all // part, act, 0)
    loads[2].wait()

    def down(q, rank):
        return dot(hid[q * part : (q + 1) * part], wd[:, pl.ds(pl.multiple_of((me.t + rank) % 4 * cols, cols), cols)])

    def send_far(q):
        far[q] = down(q, 2).astype(BF)
        remote(far.at[q], relay.at[q], rs_send.at[0, q], relay_sem.at[q], me.x(1 if q < 2 else 3)).start()

    def send_side(q, right, add):
        buf, dst, sem, rank = (to_r, from_l, fl_sem, 1) if right else (to_l, from_r, fr_sem, 3)
        y = down(q, rank)
        if add:
            await_bytes(relay.at[q], relay_sem.at[q])
            y = y + relay[q].astype(F32)
        buf[q] = y.astype(BF)
        remote(buf.at[q], dst.at[q], rs_send.at[1 if right else 2, q], sem.at[q], me.x(1 if right else 3)).start()

    def finish(q):
        y = down(q, 0)
        await_bytes(from_l.at[q], fl_sem.at[q])
        await_bytes(from_r.at[q], fr_sem.at[q])
        y = (y + from_l[q].astype(F32) + from_r[q].astype(F32)).astype(BF)
        ext = dot(pk_extra[...], y[:, 3 * 128 :])
        packed = dot(pk_main[...], y[:, : 3 * 128]) + jnp.concatenate([ext[256 * j : 256 * (j + 1)] for j in range(3)], axis=1)
        retb[2 * q : 2 * q + 2] = packed.astype(BF).reshape(2, SRC, MSG, 3 * 128)
        mine_e = me.z * SRC + me.s8
        for o in (2 * q, 2 * q + 1):
            z = (me.z - me.row(o) + n_z) % n_z

            def send(i, _):
                s = (me.s8 + i) % SRC
                remote(retb.at[o, s], reti.at[mine_e], ret_send, ret_sem, me.at(z, s)).start()
                return 0

            lax.fori_loop(1 if o == 0 else 0, SRC, send, 0)
        if q == 0:
            pltpu.make_async_copy(retb.at[0, me.s8], reti.at[mine_e], ret_sem).start()

    for first in (0, 1):
        send_far(first)
        send_far(first + 2)
        send_side(first + 2, True, False)
        send_side(first, False, False)
        for slot in (1 + first, 1 + UP + first):
            att.arrive(slot)
        for slot in (1 + first, 1 + UP + first):
            att.attend(slot)
        send_side(first, True, True)
        send_side(first + 2, False, True)
    for slot in (3, 3 + UP):
        att.arrive(slot)
    for slot in (3, 3 + UP):
        att.attend(slot)
    finish(0)
    finish(2)
    att.arrive(4)
    att.attend(4)
    att.send_sums()
    finish(1)
    finish(3)
    att.finish()

    await_bytes(reti, ret_sem)
    res = reti[...].reshape(64 * MSG, 3 * 128)
    mixed = dot(wmix[0, 0], res) + dot(wmix[0, 1], res)
    last = jnp.zeros((n_rows, 128), F32)
    for j in range(3):
        piece = res[:, 128 * j : 128 * (j + 1)]
        last = last + dot(wmix[1 + j, 0], piece) + dot(wmix[1 + j, 1], piece)
    fino[:, :, : 3 * 128] = mixed.astype(BF).reshape(4, quarter, 3 * 128)
    fino[:, :, 3 * 128 :] = last.astype(BF).reshape(4, quarter, 128)
    for step in (1, 2, 3):
        remote(fino.at[(me.t + step) % 4], fini.at[step - 1], fin_send.at[step - 1], fin_sem.at[step - 1], me.x(step)).start()
    out[:, mine] = fino[me.t]
    for step in (1, 2, 3):
        await_bytes(fini.at[step - 1], fin_sem.at[step - 1])
        theirs = pl.ds(pl.multiple_of((me.t + 4 - step) % 4 * cols, cols), cols)
        out[:, theirs] = fini[step - 1]

    for step in (0, 1, 2):
        await_bytes(fini.at[step], fin_send.at[step])
    for q in range(4):
        for k in range(3):
            await_bytes(far.at[q], rs_send.at[k, q])
    for b, k, n in ((0, 0, n_z), (0, 1, n_z), (1, 0, n_z // 2), (2, 1, n_z // 2)):
        await_bytes(arr.at[b, pl.ds(0, n)], xs_sem.at[b, k])
    for buf, sem in ((outb, out_sem), (retb, ret_send)):
        await_bytes(buf.at[pl.ds(1, n_z - 1)], sem)
        await_bytes(buf.at[0, pl.ds(1, SRC - 1)], sem)
    att.drain()


NEAR = 256


def rope_constants(n_places):
    freqs = 1.0 / THETA ** (np.arange(0, ROPE, 2, dtype=np.float64) / ROPE)
    freqs = np.tile(freqs.astype(np.float32).astype(np.float64), 4)
    table = lambda at: jnp.asarray(np.stack([np.cos(at[:, None] * freqs), np.sin(at[:, None] * freqs)]), F32)
    return table(np.arange(NEAR)), table(np.arange(n_places) * NEAR)


def on_device(
    queries,
    kv_latent,
    rope_key,
    latent_gain,
    w_key_up,
    w_value_up,
    query_gain,
    key_gain,
    rope_gain,
    out_gain,
    moe_tokens,
    moe_gain,
    routes,
    route_weights,
    w_gate,
    w_up,
    w_down,
):
    n_z = lax.axis_size("ep_0")
    n_rows, model = moe_tokens.shape
    ff = w_gate.shape[2]
    cols = model // 4
    row = lambda g: g.reshape(1, -1)
    vm = pl.BlockSpec(memory_space=pltpu.VMEM)
    hbm = pl.BlockSpec(memory_space=pl.ANY)
    chunk = (4, 192, cols)
    dma = pltpu.SemaphoreType.DMA
    slots = n_z * SRC * CAP
    return pl.pallas_call(
        functools.partial(whole_kernel, n_z),
        out_shape=(
            jax.ShapeDtypeStruct((n_rows, 2 * HEAD), BF),
            jax.ShapeDtypeStruct((n_rows // 4, model), BF),
        ),
        in_specs=[vm] * 20 + [hbm] * 3,
        out_specs=(vm, vm),
        scratch_shapes=[
            pltpu.VMEM((model, ff), BF),
            pltpu.VMEM((model, ff), BF),
            pltpu.VMEM((ff, model), BF),
            pltpu.VMEM((n_rows, cols), BF),
            pltpu.VMEM((n_z, SRC, MSG, 384), BF),
            pltpu.VMEM((4, n_z, SRC, MSG, 384), BF),
            pltpu.VMEM((4, slots, cols), BF),
            pltpu.VMEM((slots, ff), F32),
            pltpu.VMEM((slots, ff), F32),
            pltpu.VMEM((slots, ff), BF),
            pltpu.VMEM((4, 2, n_rows, 64 * MSG), BF),
            pltpu.VMEM(chunk, BF),
            pltpu.VMEM(chunk, BF),
            pltpu.VMEM(chunk, BF),
            pltpu.VMEM(chunk, BF),
            pltpu.VMEM(chunk, BF),
            pltpu.VMEM(chunk, BF),
            pltpu.VMEM((n_z, SRC, MSG, 384), BF),
            pltpu.VMEM((n_z * SRC, MSG, 384), BF),
            pltpu.VMEM((4, n_rows // 4, cols), BF),
            pltpu.VMEM((3, n_rows // 4, cols), BF),
            dma((3,)),
            dma((n_z,)),
            dma,
            dma((3, 2)),
            dma((3, n_z)),
            dma((3, 4)),
            dma((4,)),
            dma((4,)),
            dma((4,)),
            dma,
            dma,
            dma((3,)),
            dma((3,)),
            *att_scratch(),
        ],
        compiler_params=pltpu.CompilerParams(collective_id=1, has_side_effects=True, vmem_limit_bytes=62 * 1024 * 1024),
        name="layer",
    )(
        queries,
        kv_latent,
        rope_key,
        row(latent_gain),
        w_key_up,
        w_value_up,
        row(query_gain),
        row(key_gain),
        row(rope_gain),
        row(out_gain),
        *rope_constants(n_z * SRC),
        moe_tokens,
        row(moe_gain),
        routes.T,
        route_weights.T,
        *fixed_selects(),
        w_gate,
        w_up,
        w_down,
    )


def solution(mesh):
    finer = Mesh(mesh.devices.reshape(8, 4, 2, mesh.shape["tp"]), ("ep_0", "ep_1", "ep_2", "tp"))
    placed = (
        P(EP, "tp"),
        P(EP, None),
        P(EP, None),
        P(),
        P(None, "tp"),
        P(None, "tp"),
        P(),
        P(),
        P(),
        P(),
        P(EP, None),
        P(),
        P(EP, None),
        P(EP, None),
        P(EP, None, "tp"),
        P(EP, None, "tp"),
        P(EP, "tp", None),
    )
    return jax.shard_map(
        on_device,
        mesh=finer,
        in_specs=placed,
        out_specs=(P(EP, "tp"), P(EP_TP, None)),
        check_vma=False,
    )
```

```python
import functools
import math

import jax
import jax.numpy as jnp
import numpy as np
from jax import lax
from jax.experimental import pallas as pl
from jax.experimental.pallas import tpu as pltpu
from jax.sharding import Mesh
from jax.sharding import PartitionSpec as P

BF, F32, I32 = jnp.bfloat16, jnp.float32, jnp.int32
MESH = pl.DeviceIdType.MESH
Z_ORDER = (0, 1, 7, 4, 3, 5, 2, 6)

EP = ("ep_0", "ep_1", "ep_2")
EP_TP = ("ep_0", "ep_1", "ep_2", "tp")


EPS = 1e-06
THETA = 500000.0


SRC = 8
MSG = 16
CAP = 12


def split_two(v):
    hi = v.astype(BF)
    return hi, (v - hi.astype(F32)).astype(BF)


def fixed_selects():
    packed = np.arange(16 * MSG)
    slot = np.arange(16 * CAP)
    src, s = slot // CAP, slot % CAP
    main = (src * MSG + s)[:, None] == packed[None, :]
    extra = [((src * MSG + CAP + s % 4)[:, None] == packed[None, :]) & (s // 4 == j)[:, None] for j in range(3)]
    unpack_extra = np.concatenate(extra, axis=1)
    pack_extra = np.concatenate([e.T for e in extra], axis=0)
    return [jnp.asarray(a.astype(np.float32), BF) for a in (main, unpack_extra, main.T, pack_extra)]


class Place:
    def __init__(self, n_z):
        self.n_z = n_z
        self.z = lax.axis_index("ep_0")
        self.y = lax.axis_index("ep_1")
        self.c = lax.axis_index("ep_2")
        self.t = lax.axis_index("tp")
        self.s8 = self.y * 2 + self.c

    def row(self, order):
        return sum(jnp.where(order == k, d, 0) for k, d in enumerate(Z_ORDER))

    def x(self, step):
        return (self.z, self.y, self.c, (self.t + step) % 4)

    def at(self, z, s8):
        return (z, s8 // 2, s8 % 2, self.t)


def greet(pl_, n_z):
    barrier = pltpu.get_barrier_semaphore()

    def one(i, _):
        z, s = (pl_.z + i // SRC) % n_z, (pl_.s8 + i % SRC) % SRC
        pl.semaphore_signal(barrier, inc=1, device_id=pl_.at(z, s), device_id_type=MESH)
        return 0

    lax.fori_loop(1, n_z * SRC, one, 0)
    for step in (1, 2, 3):
        pl.semaphore_signal(barrier, inc=1, device_id=pl_.x(step), device_id_type=MESH)


def met(n_z):
    pl.semaphore_wait(pltpu.get_barrier_semaphore(), n_z * SRC - 1 + 3)


def remote(src, dst, send, recv, device):
    return pltpu.make_async_remote_copy(
        src_ref=src, dst_ref=dst, send_sem=send, recv_sem=recv, device_id=device, device_id_type=MESH
    )


def await_bytes(ref, sem):
    pltpu.make_async_copy(ref, ref, sem).wait()


def dot(a, b):
    return jnp.dot(a, b, preferred_element_type=F32)


HEAD = 128
ROPE = 64
PIECE = 512
HOP_AT, QUERY_AT, FIRST_AT, PAIR_AT, SUMS_AT = 1, 1, 2, 2, 6
UP, DOWN = 3, 4


class Attention:
    def __init__(self, n_z, me, ins, out, buf, sem):
        self.n_z, self.me, self.ins, self.out, self.buf, self.sem = n_z, me, ins, out, buf, sem

    def prepare(self):
        me = self.me
        (queries, kv_latent, rope_key, lat_gain, wk, wv, q_gain, key_gain, rope_gain, _, near, far) = self.ins
        twice = lambda a: jnp.concatenate([a, a], axis=-1)
        qn_gain, qr_gain = q_gain[:, :HEAD], twice(q_gain[:, HEAD:])
        place = me.z * SRC + me.s8
        far_cos, far_sin = far[0, pl.ds(place, 1)], far[1, pl.ds(place, 1)]
        cos2 = near[0] * far_cos - near[1] * far_sin
        sin2 = near[1] * far_cos + near[0] * far_sin
        kv, rk, kvb, rkb, q_all, qb = (self.buf[k] for k in ("kv", "rk", "kvb", "rkb", "q_all", "qb"))
        n = queries.shape[0]
        lane = lax.broadcasted_iota(I32, (n, 128), 1)
        low = lane < ROPE
        signed = jnp.where(lane % ROPE < ROPE // 2, -sin2, sin2)

        def turned(v):
            other = jnp.where(lane % ROPE < ROPE // 2, pltpu.roll(v, 128 - ROPE // 2, 1), pltpu.roll(v, ROPE // 2, 1))
            return v * cos2 + other * signed

        v = kv_latent[...].astype(F32)
        latent = (v * lax.rsqrt(jnp.mean(v * v, axis=-1, keepdims=True) + EPS) * lat_gain[...]).astype(BF)
        keys = dot(latent, wk[...])
        vals = dot(latent, wv[...]).astype(BF)
        for h in (0, 1):
            k = keys[:, HEAD * h : HEAD * (h + 1)]
            k = k * lax.rsqrt(jnp.mean(k * k, axis=-1, keepdims=True) + EPS) * key_gain[...]
            kvb[h, :, :HEAD] = k.astype(BF)
            kvb[h, :, HEAD:] = vals[:, HEAD * h : HEAD * (h + 1)]
        flat = rope_key[...].astype(F32)
        r = jnp.transpose(jnp.concatenate([flat, flat], axis=0))
        r = turned(r * lax.rsqrt(jnp.mean(r * r, axis=-1, keepdims=True) + EPS) * twice(rope_gain[...]))
        rkb[...] = jnp.where(low[: n // 2], r[: n // 2], r[n // 2 :]).astype(BF)

        t0, t1, t2 = (queries[:, 128 * j : 128 * (j + 1)].astype(F32) for j in range(3))
        total = lambda a: jnp.sum(a, axis=-1, keepdims=True)
        s1 = t1 * t1
        width = HEAD + ROPE
        inv0 = lax.rsqrt((total(t0 * t0) + total(jnp.where(low, s1, 0.0))) / width + EPS)
        inv1 = lax.rsqrt((total(t2 * t2) + total(jnp.where(low, 0.0, s1))) / width + EPS)
        nope1 = jnp.where(low, pltpu.roll(t1, ROPE, 1), pltpu.roll(t2, ROPE, 1))
        turn = turned(jnp.where(low, t1 * inv0, t2 * inv1) * qr_gain)
        qb[0, :, :HEAD] = (t0 * inv0 * qn_gain).astype(BF)
        qb[1, :, :HEAD] = (nope1 * inv1 * qn_gain).astype(BF)
        qb[0, :, HEAD:] = jnp.where(low, turn, 0.0).astype(BF)
        qb[1, :, HEAD:] = jnp.where(low, 0.0, turn).astype(BF)
        q_all[me.s8] = qb[me.c]
        kv[0, self.mine(256)] = kvb[me.c]
        rk[0, self.mine(128)] = rkb[...]

    def mine(self, n):
        return pl.ds(pl.multiple_of(self.me.c * n, n), n)

    def send_first(self):
        me, b, s = self.me, self.buf, self.sem
        other = (me.z, me.y, 1 - me.c, me.t)
        remote(b["kvb"].at[1 - me.c], b["kv"].at[0, self.mine(256)], s["kv_out"].at[0], s["kv_in"].at[0], other).start()
        remote(b["rkb"], b["rk"].at[0, self.mine(128)], s["kv_out"].at[1], s["rk_in"].at[0], other).start()

    def send_queries(self):
        me, b, s = self.me, self.buf, self.sem

        def one(i, _):
            d = (me.s8 + i) % SRC
            remote(b["qb"].at[d % 2], b["q_all"].at[me.s8], s["q_out"], s["q_in"], me.at(me.z, d)).start()
            return 0

        lax.fori_loop(1, SRC, one, 0)

    def first_in(self):
        b, s = self.buf, self.sem
        await_bytes(b["kvb"].at[0], s["kv_in"].at[0])
        await_bytes(b["rkb"], s["rk_in"].at[0])

    def queries_in(self):
        await_bytes(self.buf["q_all"].at[pl.ds(0, SRC - 1)], self.sem["q_in"])

    def has(self, slot):
        z = self.me.z
        return jnp.where(slot <= UP, z >= slot, (z + slot - UP) % self.n_z < DOWN)

    def uses(self, slot):
        z = self.me.z
        return jnp.where(slot <= UP, z >= slot, z + slot - UP >= self.n_z)

    def sends(self, slot, up):
        z = self.me.z
        if up:
            return (z <= self.n_z - 2) & (z >= slot) & (slot < UP)
        back = jnp.where(slot == 0, 0, slot - UP)
        return ((z + back) % self.n_z < DOWN) & ((slot == 0) | ((slot > UP) & (slot < UP + DOWN)))

    def _copies(self, slot, up):
        me, b, s = self.me, self.buf, self.sem
        to = slot + 1 if up else jnp.where(slot == 0, UP + 1, slot + 1)
        z = (me.z + (1 if up else self.n_z - 1)) % self.n_z
        where = (z, me.y, me.c, me.t)
        return (
            remote(b["kv"].at[slot], b["kv"].at[to], s["hop_out"].at[to, 0], s["kv_in"].at[to], where),
            remote(b["rk"].at[slot], b["rk"].at[to], s["hop_out"].at[to, 1], s["rk_in"].at[to], where),
        )

    def hop(self, slot, up):
        @pl.when(self.sends(slot, up))
        def _():
            for copy in self._copies(slot, up):
                copy.start()

    def arrive(self, slot):
        b, s = self.buf, self.sem

        @pl.when(self.has(slot))
        def _():
            await_bytes(b["kv"].at[slot], s["kv_in"].at[slot])
            await_bytes(b["rk"].at[slot], s["rk_in"].at[slot])

        self.hop(slot, True)
        self.hop(slot, False)

    def pairs(self, j, done):
        def arrive(side, _):
            slot = j + side * UP

            @pl.when((slot < 8) & ((side == 1) | (slot <= UP)))
            def _():
                self.arrive(slot)

            return 0

        def attend(side, _):
            slot = j + side * UP

            @pl.when((slot < 8) & ((side == 1) | (slot <= UP)) & self.uses(slot))
            def _():
                self.attend(slot, False)

            return 0

        lax.fori_loop(0, 2, attend if done else arrive, 0)

    def attend(self, slot, diagonal):
        self.load(slot)
        q_all, acc, kop, vop = (self.buf[k] for k in ("q_all", "acc", "kop", "vop"))
        n_keys = kop.shape[0]
        scale = (HEAD + ROPE) ** (-0.5) * math.log2(math.e)
        keys, vals = kop[...], vop[...]
        count, per = SRC * 256 // PIECE, PIECE // 256

        def score(m):
            q = q_all[per * m : per * (m + 1)].reshape(PIECE, 2 * HEAD)
            return lax.dot_general(q, keys, (((1,), (1,)), ((), ())), preferred_element_type=F32)

        def weigh(m, s):
            e = jnp.exp2(s * scale)
            if diagonal:
                at_q = lax.broadcasted_iota(I32, (PIECE, n_keys), 0) + m * PIECE
                at_k = lax.broadcasted_iota(I32, (PIECE, n_keys), 1) + self.me.y * n_keys
                e = jnp.where(at_q >= at_k, e, 0.0)
            got = dot(e.astype(BF), vals).reshape(per, 256, 2 * HEAD)
            if diagonal:
                acc[per * m : per * (m + 1)] = got
            else:
                acc[per * m : per * (m + 1)] += got

        s = score(0)
        for m in range(count):
            ahead = score(m + 1) if m + 1 < count else None
            weigh(m, s)
            s = ahead

    def load(self, slot):
        kv, rk, kop, vop = (self.buf[k] for k in ("kv", "rk", "kop", "vop"))
        packed = rk[slot].astype(F32)
        rolled = pltpu.roll(packed, ROPE, 1)
        low = lax.broadcasted_iota(I32, packed.shape, 1) < ROPE
        lo = jnp.where(low, packed, rolled).astype(BF)
        hi = jnp.where(low, rolled, packed).astype(BF)
        kop[:, :HEAD] = kv[slot, :, :HEAD]
        for half in (0, 1):
            kop[256 * half : 256 * half + 128, HEAD:] = lo[128 * half : 128 * half + 128]
            kop[256 * half + 128 : 256 * half + 256, HEAD:] = hi[128 * half : 128 * half + 128]
        vop[:, :HEAD] = kv[slot, :, HEAD:]

    def ones(self):
        vop = self.buf["vop"]
        vop[:, HEAD:] = jnp.ones((vop.shape[0], HEAD), BF)

    def send_sums(self):
        me, b, s = self.me, self.buf, self.sem
        acc, ob, db, od, dd = (b[k] for k in ("acc", "ob", "db", "od", "dd"))

        def halves(m):
            a = acc[m]
            return a[:, :HEAD].astype(BF), jnp.transpose(a[:, HEAD:])[:8]

        def one(i, _):
            m = (me.s8 + i) % SRC
            ob[m], db[m] = halves(m)
            where = me.at(me.z, m)
            remote(ob.at[m], od.at[me.s8], s["o_out"].at[0], s["o_in"].at[0], where).start()
            remote(db.at[m], dd.at[me.s8], s["o_out"].at[1], s["o_in"].at[1], where).start()
            return 0

        lax.fori_loop(1, SRC, one, 0)
        od[me.s8], dd[me.s8] = halves(me.s8)

    def finish(self):
        b, s = self.buf, self.sem
        od, dd = b["od"], b["dd"]
        out_gain = self.ins[9]
        await_bytes(od.at[pl.ds(0, SRC - 1)], s["o_in"].at[0])
        await_bytes(dd.at[pl.ds(0, SRC - 1)], s["o_in"].at[1])
        for h in (0, 1):
            o = sum(od[2 * y + h].astype(F32) for y in range(4))
            d = sum(dd[2 * y + h] for y in range(4))
            den = jnp.transpose(jnp.broadcast_to(d[0:1], (HEAD, d.shape[1])))
            m = o / den
            m = m * lax.rsqrt(jnp.mean(m * m, axis=-1, keepdims=True) + EPS) * out_gain[...]
            self.out[:, HEAD * h : HEAD * (h + 1)] = m.astype(BF)

    def drain(self):
        b, s = self.buf, self.sem
        await_bytes(b["kvb"].at[0], s["kv_out"].at[0])
        await_bytes(b["rkb"], s["kv_out"].at[1])
        await_bytes(b["q_all"].at[pl.ds(0, SRC - 1)], s["q_out"])
        for slot, up in [(k, True) for k in range(UP)] + [(0, False)] + [(UP + k, False) for k in range(1, DOWN)]:

            @pl.when(self.sends(slot, up))
            def _():
                for copy in self._copies(slot, up):
                    copy.wait_send()

        await_bytes(b["od"].at[pl.ds(0, SRC - 1)], s["o_out"].at[0])
        await_bytes(b["dd"].at[pl.ds(0, SRC - 1)], s["o_out"].at[1])


ATT_BUFS = {
    "kv": ((8, 512, 256), "bf"),
    "rk": ((8, 256, 128), "bf"),
    "kvb": ((2, 256, 256), "bf"),
    "rkb": ((128, 128), "bf"),
    "q_all": ((8, 256, 256), "bf"),
    "qb": ((2, 256, 256), "bf"),
    "acc": ((8, 256, 256), "f"),
    "kop": ((512, 256), "bf"),
    "vop": ((512, 256), "bf"),
    "ob": ((8, 256, 128), "bf"),
    "db": ((8, 8, 256), "f"),
    "od": ((8, 256, 128), "bf"),
    "dd": ((8, 8, 256), "f"),
}
ATT_SEMS = {"kv_out": (2,), "kv_in": (8,), "rk_in": (8,), "q_out": None, "q_in": None, "hop_out": (8, 2), "o_out": (2,), "o_in": (2,)}


def att_scratch():
    bufs = [pltpu.VMEM(shape, BF if kind == "bf" else F32) for shape, kind in ATT_BUFS.values()]
    sems = [pltpu.SemaphoreType.DMA if n is None else pltpu.SemaphoreType.DMA(n) for n in ATT_SEMS.values()]
    return bufs + sems


def att_refs(refs):
    n = len(ATT_BUFS)
    return dict(zip(ATT_BUFS, refs[:n])), dict(zip(ATT_SEMS, refs[n:]))


BIG = ("tokens", "queries", "kv_latent", "w_key", "w_val", "near", "un_main", "un_extra", "pk_main", "pk_extra")
OWN = (
    "wgu",
    "wd",
    "normed",
    "outb",
    "arr",
    "rows",
    "hid",
    "wmix",
    "far",
    "to_r",
    "to_l",
    "relay",
    "from_l",
    "from_r",
    "retb",
    "reti",
    "fino",
    "fini",
    "w_sem",
    "own_sem",
    "out_sem",
    "xs_sem",
    "xr_sem",
    "rs_send",
    "relay_sem",
    "fl_sem",
    "fr_sem",
    "ret_send",
    "ret_sem",
    "fin_send",
    "fin_sem",
)


def whole_kernel(n_z, *refs):
    n_small, n_big, n_own = 10, len(BIG), len(OWN)
    (lat_gain, q_gain, key_gain, rope_gain, out_gain, far_table, rope_key, gain, routes_t, weights_t) = refs[:n_small]
    refs = refs[n_small:]
    big_hbm, (wg_hbm, wu_hbm, wd_hbm), refs = refs[:n_big], refs[n_big : n_big + 3], refs[n_big + 3 :]
    a_out, out, refs = refs[0], refs[1], refs[2:]
    own = dict(zip(OWN, refs[:n_own]))
    big, big_sem, refs = refs[n_own : n_own + n_big], refs[n_own + n_big], refs[n_own + n_big + 1 :]
    (tokens, queries, kv_latent, w_key, w_val, near_table, un_main, un_extra, pk_main, pk_extra) = big
    takes = [pltpu.make_async_copy(h, v, big_sem.at[k]) for k, (h, v) in enumerate(zip(big_hbm, big))]
    for take in takes:
        take.start()
    a_in = (queries, kv_latent, rope_key, lat_gain, w_key, w_val, q_gain, key_gain, rope_gain, out_gain, near_table, far_table)
    wgu, wd, normed, outb, arr, rows = (own[k] for k in ("wgu", "wd", "normed", "outb", "arr", "rows"))
    hid, wmix, far, to_r, to_l, relay = (own[k] for k in ("hid", "wmix", "far", "to_r", "to_l", "relay"))
    from_l, from_r, retb, reti, fino, fini = (own[k] for k in ("from_l", "from_r", "retb", "reti", "fino", "fini"))
    w_sem, own_sem, out_sem, xs_sem, xr_sem, rs_send = (own[k] for k in ("w_sem", "own_sem", "out_sem", "xs_sem", "xr_sem", "rs_send"))
    relay_sem, fl_sem, fr_sem, ret_send, ret_sem, fin_send = (own[k] for k in ("relay_sem", "fl_sem", "fr_sem", "ret_send", "ret_sem", "fin_send"))
    fin_sem = own["fin_sem"]
    me = Place(n_z)
    att = Attention(n_z, me, a_in, a_out, *att_refs(refs))
    greet(me, n_z)
    ff = wd.shape[0]
    loads = [
        pltpu.make_async_copy(wg_hbm.at[0], wgu.at[:, pl.ds(0, ff)], w_sem.at[0]),
        pltpu.make_async_copy(wu_hbm.at[0], wgu.at[:, pl.ds(ff, ff)], w_sem.at[1]),
        pltpu.make_async_copy(wd_hbm.at[0], wd, w_sem.at[2]),
    ]
    for load in loads:
        load.start()
    n_rows, model = tokens.shape
    cols = model // 4
    quarter = n_rows // 4

    exp_ids = lax.broadcasted_iota(I32, (64, n_rows), 0)
    ra, rb = routes_t[0:1, :], routes_t[1:2, :]
    hit_a, hit_b = exp_ids == ra, exp_ids == rb
    both = jnp.where(hit_a | hit_b, 1.0, 0.0).astype(BF)
    i0 = lax.broadcasted_iota(I32, (n_rows, n_rows), 0)
    i1 = lax.broadcasted_iota(I32, (n_rows, n_rows), 1)
    same = (i0 // quarter) == (i1 // quarter)
    earlier_t = jnp.where((i0 < i1) & same, 1.0, 0.0).astype(BF)
    count_t = dot(both, earlier_t)
    base_t = lax.broadcasted_iota(I32, (1, n_rows), 1) // quarter * 3

    def places(hit, chosen):
        s = base_t + jnp.sum(jnp.where(hit, count_t, 0.0), axis=0, keepdims=True).astype(I32)
        return chosen * MSG + s, chosen * MSG + CAP + s % 4 + 2048 * (s // 4)

    (ma, xa), (mb, xb) = places(hit_a, ra), places(hit_b, rb)

    takes[0].wait()
    v = tokens[...].astype(F32)
    scale = lax.rsqrt(jnp.mean(v * v, axis=-1, keepdims=True) + EPS)
    mine = pl.ds(pl.multiple_of(me.t * cols, cols), cols)
    normed[...] = (tokens[:, mine].astype(F32) * scale * gain[:, mine]).astype(BF)

    met(n_z)

    def dispatch(o, _):
        z = (me.z + me.row(o)) % n_z
        first = z * SRC * MSG
        ids = lax.broadcasted_iota(I32, (SRC * MSG, n_rows), 0) + first
        main = jnp.where((ids == ma) | (ids == mb), 1.0, 0.0).astype(BF)
        block = dot(main, normed[:, : 3 * 128])
        extra = []
        for j in range(3):
            idj = ids + 2048 * j
            sel = jnp.where((idj == xa) | (idj == xb), 1.0, 0.0).astype(BF)
            extra.append(dot(sel, normed[:, 3 * 128 :]))
        block = block + jnp.concatenate(extra, axis=1)
        outb[o] = block.astype(BF).reshape(SRC, MSG, 3 * 128)

        def send(i, _):
            s = (me.s8 + i) % SRC
            remote(outb.at[o, s], arr.at[0, o, me.s8], out_sem, own_sem.at[o], me.at(z, s)).start()
            return 0

        lax.fori_loop(jnp.where(o == 0, 1, 0), SRC, send, 0)
        return 0

    lax.fori_loop(0, n_z, dispatch, 0)
    pltpu.make_async_copy(outb.at[0, me.s8], arr.at[0, 0, me.s8], own_sem.at[0]).start()

    upright = lambda row: jnp.transpose(jnp.broadcast_to(row, (128, n_rows)))[:, 0:1]
    lane_e = lax.broadcasted_iota(I32, (n_rows, 128), 1)
    ca, cb = (upright(r.astype(F32)).astype(I32) for r in (ra, rb))
    on_a, on_b = lane_e == ca, lane_e == cb
    earlier = jnp.where((i1 < i0) & same, 1.0, 0.0).astype(BF)
    count = dot(earlier, jnp.where(on_a | on_b, 1.0, 0.0).astype(BF))
    base = lax.broadcasted_iota(I32, (n_rows, 1), 0) // quarter * 3
    wa, wb = (upright(weights_t[k : k + 1, :]) for k in (0, 1))

    def places_c(hit, chosen):
        s = base + jnp.sum(jnp.where(hit, count, 0.0), axis=1, keepdims=True).astype(I32)
        return chosen * MSG + s, chosen * MSG + CAP + s % 4 + 2048 * (s // 4)

    (cma, cxa), (cmb, cxb) = places_c(on_a, ca), places_c(on_b, cb)

    def mix(k, _):
        lanes = lax.broadcasted_iota(I32, (n_rows, 64 * MSG), 1)
        idk = lanes + 2048 * (k - 1)
        pa, pb = jnp.where(k == 0, cma - 2048, cxa), jnp.where(k == 0, cmb - 2048, cxb)
        w = jnp.where(idk == pa, wa, 0.0) + jnp.where(idk == pb, wb, 0.0)
        hi, lo = split_two(w)
        wmix[k, 0] = hi
        wmix[k, 1] = lo
        return 0


    def pass_on(b, o, step, dst):
        remote(arr.at[b, o], arr.at[dst, o], xs_sem.at[b, step % 4 // 2], xr_sem.at[dst - 1, o], me.x(step)).start()

    def rank_cols(rank, width=cols, skip=0):
        return pl.ds(pl.multiple_of((me.t + rank) % 4 * cols + skip, 128), width)

    def unpack(b, rank, p):
        packed = arr[b, pl.ds(2 * p, 2)].reshape(2 * SRC * MSG, 3 * 128)
        tiles = jnp.concatenate([packed[:, 128 * j : 128 * (j + 1)] for j in range(3)], axis=0)
        rows[:, rank_cols(rank, 3 * 128)] = dot(un_main[...], packed).astype(BF)
        rows[:, rank_cols(rank, 128, 3 * 128)] = dot(un_extra[...], tiles).astype(BF)

    def unpack_near(p):
        for b, rank in ((0, 0), (1, 3), (2, 1)):
            unpack(b, rank, p)

    def gather(o):
        await_bytes(arr.at[0, o], own_sem.at[o])
        pass_on(0, o, 1, 1)
        pass_on(0, o, 3, 2)

    def relay_on(o):
        await_bytes(arr.at[1, o], xr_sem.at[0, o])
        await_bytes(arr.at[2, o], xr_sem.at[1, o])

        @pl.when(o % 2 == 0)
        def _():
            pass_on(1, o, 1, 3)

        @pl.when(o % 2 == 1)
        def _():
            pass_on(2, o, 3, 3)

    def down(q, rank):
        return dot(hid[q], wd[:, rank_cols(rank)])

    half = 96
    parts = (pl.ds(0, half), pl.ds(half, half))

    def hidden_units(p):
        await_bytes(arr.at[3, 2 * p], xr_sem.at[2, 2 * p])
        await_bytes(arr.at[3, 2 * p + 1], xr_sem.at[2, 2 * p + 1])
        unpack(3, 2, p)
        gu = dot(rows[...], wgu[...])
        g, u = gu[:, :ff], gu[:, ff:]
        hid[p] = (g / (1.0 + jnp.exp(-g)) * u).astype(BF)
        far[p] = down(p, 2).astype(BF)
        for k, step in ((0, 1), (1, 3)):
            remote(far.at[p, parts[k]], relay.at[p, parts[k]], rs_send.at[0, p, k], relay_sem.at[p, k], me.x(step)).start()

    def sides(q):
        await_bytes(relay.at[q, parts[0]], relay_sem.at[q, 0])
        await_bytes(relay.at[q, parts[1]], relay_sem.at[q, 1])
        for k, (buf, dst, sem, rank) in enumerate(((to_r, from_l, fl_sem, 1), (to_l, from_r, fr_sem, 3))):
            y = down(q, rank)
            added = y[half * k : half * (k + 1)] + relay[q, parts[k]].astype(F32)
            kept = y[half * (1 - k) : half * (2 - k)]
            buf[q, parts[k]] = added.astype(BF)
            buf[q, parts[1 - k]] = kept.astype(BF)
            remote(buf.at[q], dst.at[q], rs_send.at[1 + k, q, 0], sem.at[q], me.x(rank)).start()

    def finish(q):
        y = down(q, 0)
        await_bytes(from_l.at[q], fl_sem.at[q])
        await_bytes(from_r.at[q], fr_sem.at[q])
        y = (y + from_l[q].astype(F32) + from_r[q].astype(F32)).astype(BF)
        ext = dot(pk_extra[...], y[:, 3 * 128 :])
        packed = dot(pk_main[...], y[:, : 3 * 128]) + jnp.concatenate([ext[256 * j : 256 * (j + 1)] for j in range(3)], axis=1)
        retb[pl.ds(2 * q, 2)] = packed.astype(BF).reshape(2, SRC, MSG, 3 * 128)
        mine_e = me.z * SRC + me.s8

        def send(i, _):
            o = 2 * q + i // SRC
            z = (me.z - me.row(o) + n_z) % n_z
            s = (me.s8 + i) % SRC
            remote(retb.at[o, s], reti.at[mine_e], ret_send, ret_sem, me.at(z, s)).start()
            return 0

        lax.fori_loop(jnp.where(q == 0, 1, 0), 2 * SRC, send, 0)

        @pl.when(q == 0)
        def _():
            pltpu.make_async_copy(retb.at[0, me.s8], reti.at[mine_e], ret_sem).start()

    n_pairs = n_z // 2

    def step(k, _):
        @pl.when(k < n_pairs)
        def _():
            gather(2 * k)

            @pl.when(k == 0)
            def _():
                for take in takes[1:]:
                    take.wait()
                att.prepare()
                att.ones()
                att.send_first()
                lax.fori_loop(0, 4, mix, 0)

            @pl.when(k > 0)
            def _():
                relay_on(2 * k - 1)
                unpack_near(k - 1)

            gather(2 * k + 1)
            relay_on(2 * k)

        @pl.when(k == n_pairs)
        def _():
            relay_on(n_z - 1)
            unpack_near(n_pairs - 1)

        @pl.when(k == QUERY_AT)
        def _():
            att.send_queries()

        @pl.when(k == HOP_AT)
        def _():
            att.first_in()
            att.hop(0, True)
            att.hop(0, False)

        @pl.when((k >= PAIR_AT) & (k < PAIR_AT + DOWN))
        def _():
            att.pairs(k - PAIR_AT + 1, False)

        @pl.when((k >= 3) & (k < n_pairs + 3))
        def _():
            finish(k - 3)

        @pl.when((k >= 2) & (k < n_pairs + 2))
        def _():
            sides(k - 2)

        @pl.when((k >= 1) & (k < n_pairs + 1))
        def _():
            @pl.when(k == 1)
            def _():
                loads[0].wait()
                loads[1].wait()
                loads[2].wait()

            hidden_units(k - 1)

        @pl.when(k == FIRST_AT)
        def _():
            att.queries_in()
            att.attend(0, True)

        @pl.when((k >= PAIR_AT) & (k < PAIR_AT + DOWN))
        def _():
            att.pairs(k - PAIR_AT + 1, True)

        @pl.when(k == jnp.where(me.z > DOWN - 1, SUMS_AT, jnp.where(me.z == 0, FIRST_AT, PAIR_AT + me.z - 1)))
        def _():
            att.send_sums()

        return 0

    lax.fori_loop(0, n_pairs + 3, step, 0)
    att.finish()

    await_bytes(reti, ret_sem)
    res = reti[...].reshape(64 * MSG, 3 * 128)
    mixed = dot(wmix[0, 0], res) + dot(wmix[0, 1], res)
    last = jnp.zeros((n_rows, 128), F32)
    for j in range(3):
        piece = res[:, 128 * j : 128 * (j + 1)]
        last = last + dot(wmix[1 + j, 0], piece) + dot(wmix[1 + j, 1], piece)
    fino[:, :, : 3 * 128] = mixed.astype(BF).reshape(4, quarter, 3 * 128)
    fino[:, :, 3 * 128 :] = last.astype(BF).reshape(4, quarter, 128)
    for step in (1, 2, 3):
        remote(fino.at[(me.t + step) % 4], fini.at[step - 1], fin_send.at[step - 1], fin_sem.at[step - 1], me.x(step)).start()
    out[:, mine] = fino[me.t]
    for step in (1, 2, 3):
        await_bytes(fini.at[step - 1], fin_sem.at[step - 1])
        theirs = pl.ds(pl.multiple_of((me.t + 4 - step) % 4 * cols, cols), cols)
        out[:, theirs] = fini[step - 1]

    for step in (0, 1, 2):
        await_bytes(fini.at[step], fin_send.at[step])
    for q in range(4):
        for k in (0, 1):
            await_bytes(far.at[q, parts[k]], rs_send.at[0, q, k])
            await_bytes(far.at[q], rs_send.at[1 + k, q, 0])
    for b, k, n in ((0, 0, n_z), (0, 1, n_z), (1, 0, n_z // 2), (2, 1, n_z // 2)):
        await_bytes(arr.at[b, pl.ds(0, n)], xs_sem.at[b, k])
    for buf, sem in ((outb, out_sem), (retb, ret_send)):
        await_bytes(buf.at[pl.ds(1, n_z - 1)], sem)
        await_bytes(buf.at[0, pl.ds(1, SRC - 1)], sem)
    att.drain()


NEAR = 256


def rope_constants(n_places):
    freqs = 1.0 / THETA ** (np.arange(0, ROPE, 2, dtype=np.float64) / ROPE)
    freqs = np.tile(freqs.astype(np.float32).astype(np.float64), 4)
    table = lambda at: jnp.asarray(np.stack([np.cos(at[:, None] * freqs), np.sin(at[:, None] * freqs)]), F32)
    return table(np.arange(NEAR)), table(np.arange(n_places) * NEAR)


def on_device(
    queries,
    kv_latent,
    rope_key,
    latent_gain,
    w_key_up,
    w_value_up,
    query_gain,
    key_gain,
    rope_gain,
    out_gain,
    moe_tokens,
    moe_gain,
    routes,
    route_weights,
    w_gate,
    w_up,
    w_down,
):
    n_z = lax.axis_size("ep_0")
    n_rows, model = moe_tokens.shape
    ff = w_gate.shape[2]
    cols = model // 4
    row = lambda g: g.reshape(1, -1)
    vm = pl.BlockSpec(memory_space=pltpu.VMEM)
    hbm = pl.BlockSpec(memory_space=pl.ANY)
    chunk = (4, 192, cols)
    near, far = rope_constants(n_z * SRC)
    small = tuple(row(g) for g in (latent_gain, query_gain, key_gain, rope_gain, out_gain))
    small += (far, rope_key.T, row(moe_gain), routes.T, route_weights.T)
    big = (moe_tokens, queries, kv_latent, w_key_up, w_value_up, near, *fixed_selects())
    dma = pltpu.SemaphoreType.DMA
    return pl.pallas_call(
        functools.partial(whole_kernel, n_z),
        out_shape=(
            jax.ShapeDtypeStruct((n_rows, 2 * HEAD), BF),
            jax.ShapeDtypeStruct((n_rows // 4, model), BF),
        ),
        in_specs=[vm] * len(small) + [hbm] * (len(big) + 3),
        out_specs=(vm, vm),
        scratch_shapes=[
            pltpu.VMEM((model, 2 * ff), BF),
            pltpu.VMEM((ff, model), BF),
            pltpu.VMEM((n_rows, cols), BF),
            pltpu.VMEM((n_z, SRC, MSG, 384), BF),
            pltpu.VMEM((4, n_z, SRC, MSG, 384), BF),
            pltpu.VMEM((192, model), BF),
            pltpu.VMEM((4, 192, ff), BF),
            pltpu.VMEM((4, 2, n_rows, 64 * MSG), BF),
            *[pltpu.VMEM(chunk, BF)] * 6,
            pltpu.VMEM((n_z, SRC, MSG, 384), BF),
            pltpu.VMEM((n_z * SRC, MSG, 384), BF),
            pltpu.VMEM((4, n_rows // 4, cols), BF),
            pltpu.VMEM((3, n_rows // 4, cols), BF),
            dma((3,)),
            dma((n_z,)),
            dma,
            dma((3, 2)),
            dma((3, n_z)),
            dma((3, 4, 2)),
            dma((4, 2)),
            dma((4,)),
            dma((4,)),
            dma,
            dma,
            dma((3,)),
            dma((3,)),
            *[pltpu.VMEM(a.shape, a.dtype) for a in big],
            dma((len(big),)),
            *att_scratch(),
        ],
        compiler_params=pltpu.CompilerParams(collective_id=1, has_side_effects=True, vmem_limit_bytes=62 * 1024 * 1024),
        name="layer",
    )(
        *small,
        *big,
        w_gate,
        w_up,
        w_down,
    )


def solution(mesh):
    finer = Mesh(mesh.devices.reshape(8, 4, 2, mesh.shape["tp"]), ("ep_0", "ep_1", "ep_2", "tp"))
    placed = (
        P(EP, "tp"),
        P(EP, None),
        P(EP, None),
        P(),
        P(None, "tp"),
        P(None, "tp"),
        P(),
        P(),
        P(),
        P(),
        P(EP, None),
        P(),
        P(EP, None),
        P(EP, None),
        P(EP, None, "tp"),
        P(EP, None, "tp"),
        P(EP, "tp", None),
    )
    return jax.shard_map(
        on_device,
        mesh=finer,
        in_specs=placed,
        out_specs=(P(EP, "tp"), P(EP_TP, None)),
        check_vma=False,
    )
```

```python
import functools
import math

import jax
import jax.numpy as jnp
import numpy as np
from jax import lax
from jax.experimental import pallas as pl
from jax.experimental.pallas import tpu as pltpu
from jax.sharding import Mesh
from jax.sharding import PartitionSpec as P

BF, F32, I32 = jnp.bfloat16, jnp.float32, jnp.int32
MESH = pl.DeviceIdType.MESH
Z_ORDER = (0, 1, 7, 4, 3, 5, 2, 6)

EP = ("ep_0", "ep_1", "ep_2")
EP_TP = ("ep_0", "ep_1", "ep_2", "tp")


EPS = 1e-06
THETA = 500000.0


SRC = 8
MSG = 16
CAP = 12


def split_two(v):
    hi = v.astype(BF)
    return hi, (v - hi.astype(F32)).astype(BF)


def fixed_selects():
    packed = np.arange(16 * MSG)
    slot = np.arange(16 * CAP)
    src, s = slot // CAP, slot % CAP
    main = (src * MSG + s)[:, None] == packed[None, :]
    extra = [((src * MSG + CAP + s % 4)[:, None] == packed[None, :]) & (s // 4 == j)[:, None] for j in range(3)]
    unpack_extra = np.concatenate(extra, axis=1)
    pack_extra = np.concatenate([e.T for e in extra], axis=0)
    return [jnp.asarray(a.astype(np.float32), BF) for a in (main, unpack_extra, main.T, pack_extra)]


class Place:
    def __init__(self, n_z):
        self.n_z = n_z
        self.z = lax.axis_index("ep_0")
        self.y = lax.axis_index("ep_1")
        self.c = lax.axis_index("ep_2")
        self.t = lax.axis_index("tp")
        self.s8 = self.y * 2 + self.c

    def row(self, order):
        return sum(jnp.where(order == k, d, 0) for k, d in enumerate(Z_ORDER))

    def x(self, step):
        return (self.z, self.y, self.c, (self.t + step) % 4)

    def at(self, z, s8):
        return (z, s8 // 2, s8 % 2, self.t)


def greet(pl_, n_z):
    barrier = pltpu.get_barrier_semaphore()

    def one(i, _):
        z, s = (pl_.z + i // SRC) % n_z, (pl_.s8 + i % SRC) % SRC
        pl.semaphore_signal(barrier, inc=1, device_id=pl_.at(z, s), device_id_type=MESH)
        return 0

    lax.fori_loop(1, n_z * SRC, one, 0)
    for step in (1, 2, 3):
        pl.semaphore_signal(barrier, inc=1, device_id=pl_.x(step), device_id_type=MESH)


def met(n_z):
    pl.semaphore_wait(pltpu.get_barrier_semaphore(), n_z * SRC - 1 + 3)


def remote(src, dst, send, recv, device):
    return pltpu.make_async_remote_copy(
        src_ref=src, dst_ref=dst, send_sem=send, recv_sem=recv, device_id=device, device_id_type=MESH
    )


def await_bytes(ref, sem):
    pltpu.make_async_copy(ref, ref, sem).wait()


def dot(a, b):
    return jnp.dot(a, b, preferred_element_type=F32)


HEAD = 128
ROPE = 64
PIECE = 512
HOP_AT, QUERY_AT, FIRST_AT, PAIR_AT = 1, 1, 2, 2
UP, DOWN = 3, 4


class Attention:
    def __init__(self, n_z, me, ins, out, buf, sem):
        self.n_z, self.me, self.ins, self.out, self.buf, self.sem = n_z, me, ins, out, buf, sem

    def prepare(self):
        me = self.me
        (queries, kv_latent, rope_key, lat_gain, wk, wv, q_gain, key_gain, rope_gain, _, near, far) = self.ins
        twice = lambda a: jnp.concatenate([a, a], axis=-1)
        qn_gain, qr_gain = q_gain[:, :HEAD], twice(q_gain[:, HEAD:])
        place = me.z * SRC + me.s8
        far_cos, far_sin = far[0, pl.ds(place, 1)], far[1, pl.ds(place, 1)]
        cos2 = near[0] * far_cos - near[1] * far_sin
        sin2 = near[1] * far_cos + near[0] * far_sin
        kv, rk, kvb, rkb, q_all, qb = (self.buf[k] for k in ("kv", "rk", "kvb", "rkb", "q_all", "qb"))
        n = queries.shape[0]
        lane = lax.broadcasted_iota(I32, (n, 128), 1)
        low = lane < ROPE
        signed = jnp.where(lane % ROPE < ROPE // 2, -sin2, sin2)

        def turned(v):
            other = jnp.where(lane % ROPE < ROPE // 2, pltpu.roll(v, 128 - ROPE // 2, 1), pltpu.roll(v, ROPE // 2, 1))
            return v * cos2 + other * signed

        v = kv_latent[...].astype(F32)
        latent = (v * lax.rsqrt(jnp.mean(v * v, axis=-1, keepdims=True) + EPS) * lat_gain[...]).astype(BF)
        keys = dot(latent, wk[...])
        vals = dot(latent, wv[...]).astype(BF)
        for h in (0, 1):
            k = keys[:, HEAD * h : HEAD * (h + 1)]
            k = k * lax.rsqrt(jnp.mean(k * k, axis=-1, keepdims=True) + EPS) * key_gain[...]
            kvb[h, :, :HEAD] = k.astype(BF)
            kvb[h, :, HEAD:] = vals[:, HEAD * h : HEAD * (h + 1)]
        flat = rope_key[...].astype(F32)
        r = jnp.transpose(jnp.concatenate([flat, flat], axis=0))
        r = turned(r * lax.rsqrt(jnp.mean(r * r, axis=-1, keepdims=True) + EPS) * twice(rope_gain[...]))
        rkb[...] = jnp.where(low[: n // 2], r[: n // 2], r[n // 2 :]).astype(BF)

        t0, t1, t2 = (queries[:, 128 * j : 128 * (j + 1)].astype(F32) for j in range(3))
        total = lambda a: jnp.sum(a, axis=-1, keepdims=True)
        s1 = t1 * t1
        width = HEAD + ROPE
        inv0 = lax.rsqrt((total(t0 * t0) + total(jnp.where(low, s1, 0.0))) / width + EPS)
        inv1 = lax.rsqrt((total(t2 * t2) + total(jnp.where(low, 0.0, s1))) / width + EPS)
        nope1 = jnp.where(low, pltpu.roll(t1, ROPE, 1), pltpu.roll(t2, ROPE, 1))
        turn = turned(jnp.where(low, t1 * inv0, t2 * inv1) * qr_gain)
        qb[0, :, :HEAD] = (t0 * inv0 * qn_gain).astype(BF)
        qb[1, :, :HEAD] = (nope1 * inv1 * qn_gain).astype(BF)
        qb[0, :, HEAD:] = jnp.where(low, turn, 0.0).astype(BF)
        qb[1, :, HEAD:] = jnp.where(low, 0.0, turn).astype(BF)
        q_all[me.s8] = qb[me.c]
        kv[0, self.mine(256)] = kvb[me.c]
        rk[0, self.mine(128)] = rkb[...]

    def mine(self, n):
        return pl.ds(pl.multiple_of(self.me.c * n, n), n)

    def send_first(self):
        me, b, s = self.me, self.buf, self.sem
        other = (me.z, me.y, 1 - me.c, me.t)
        remote(b["kvb"].at[1 - me.c], b["kv"].at[0, self.mine(256)], s["kv_out"].at[0], s["kv_in"].at[0], other).start()
        remote(b["rkb"], b["rk"].at[0, self.mine(128)], s["kv_out"].at[1], s["rk_in"].at[0], other).start()

    def send_queries(self):
        me, b, s = self.me, self.buf, self.sem

        def one(i, _):
            d = (me.s8 + i) % SRC
            remote(b["qb"].at[d % 2], b["q_all"].at[me.s8], s["q_out"], s["q_in"], me.at(me.z, d)).start()
            return 0

        lax.fori_loop(1, SRC, one, 0)

    def first_in(self):
        b, s = self.buf, self.sem
        await_bytes(b["kvb"].at[0], s["kv_in"].at[0])
        await_bytes(b["rkb"], s["rk_in"].at[0])

    def queries_in(self):
        await_bytes(self.buf["q_all"].at[pl.ds(0, SRC - 1)], self.sem["q_in"])

    def has(self, slot):
        z = self.me.z
        return jnp.where(slot <= UP, z >= slot, (z + slot - UP) % self.n_z < DOWN)

    def uses(self, slot):
        z = self.me.z
        return jnp.where(slot <= UP, z >= slot, z + slot - UP >= self.n_z)

    def sends(self, slot, up):
        z = self.me.z
        if up:
            return (z <= self.n_z - 2) & (z >= slot) & (slot < UP)
        back = jnp.where(slot == 0, 0, slot - UP)
        return ((z + back) % self.n_z < DOWN) & ((slot == 0) | ((slot > UP) & (slot < UP + DOWN)))

    def _copies(self, slot, up):
        me, b, s = self.me, self.buf, self.sem
        to = slot + 1 if up else jnp.where(slot == 0, UP + 1, slot + 1)
        z = (me.z + (1 if up else self.n_z - 1)) % self.n_z
        where = (z, me.y, me.c, me.t)
        return (
            remote(b["kv"].at[slot], b["kv"].at[to], s["hop_out"].at[to, 0], s["kv_in"].at[to], where),
            remote(b["rk"].at[slot], b["rk"].at[to], s["hop_out"].at[to, 1], s["rk_in"].at[to], where),
        )

    def hop(self, slot, up):
        @pl.when(self.sends(slot, up))
        def _():
            for copy in self._copies(slot, up):
                copy.start()

    def arrive(self, slot):
        b, s = self.buf, self.sem

        @pl.when(self.has(slot))
        def _():
            await_bytes(b["kv"].at[slot], s["kv_in"].at[slot])
            await_bytes(b["rk"].at[slot], s["rk_in"].at[slot])

        self.hop(slot, True)
        self.hop(slot, False)

    def pairs(self, j, done):
        def arrive(side, _):
            slot = j + side * UP

            @pl.when((slot < 8) & ((side == 1) | (slot <= UP)))
            def _():
                self.arrive(slot)

            return 0

        def attend(side, _):
            slot = j + side * UP

            @pl.when((slot < 8) & ((side == 1) | (slot <= UP)) & self.uses(slot))
            def _():
                self.attend(slot, False)

            return 0

        lax.fori_loop(0, 2, attend if done else arrive, 0)

    def attend(self, slot, diagonal):
        self.load(slot)
        q_all, acc, kop, vop = (self.buf[k] for k in ("q_all", "acc", "kop", "vop"))
        n_keys = kop.shape[0]
        scale = (HEAD + ROPE) ** (-0.5) * math.log2(math.e)
        keys, vals = kop[...], vop[...]
        count, per = SRC * 256 // PIECE, PIECE // 256

        def score(m):
            q = q_all[per * m : per * (m + 1)].reshape(PIECE, 2 * HEAD)
            return lax.dot_general(q, keys, (((1,), (1,)), ((), ())), preferred_element_type=F32)

        def weigh(m, s):
            e = jnp.exp2(s * scale)
            if diagonal:
                at_q = lax.broadcasted_iota(I32, (PIECE, n_keys), 0) + m * PIECE
                at_k = lax.broadcasted_iota(I32, (PIECE, n_keys), 1) + self.me.y * n_keys
                e = jnp.where(at_q >= at_k, e, 0.0)
            got = dot(e.astype(BF), vals).reshape(per, 256, 2 * HEAD)
            if diagonal:
                acc[per * m : per * (m + 1)] = got
            else:
                acc[per * m : per * (m + 1)] += got

        s = score(0)
        for m in range(count):
            ahead = score(m + 1) if m + 1 < count else None
            weigh(m, s)
            s = ahead

    def load(self, slot):
        kv, rk, kop, vop = (self.buf[k] for k in ("kv", "rk", "kop", "vop"))
        packed = rk[slot].astype(F32)
        rolled = pltpu.roll(packed, ROPE, 1)
        low = lax.broadcasted_iota(I32, packed.shape, 1) < ROPE
        lo = jnp.where(low, packed, rolled).astype(BF)
        hi = jnp.where(low, rolled, packed).astype(BF)
        kop[:, :HEAD] = kv[slot, :, :HEAD]
        for half in (0, 1):
            kop[256 * half : 256 * half + 128, HEAD:] = lo[128 * half : 128 * half + 128]
            kop[256 * half + 128 : 256 * half + 256, HEAD:] = hi[128 * half : 128 * half + 128]
        vop[:, :HEAD] = kv[slot, :, HEAD:]

    def ones(self):
        vop = self.buf["vop"]
        vop[:, HEAD:] = jnp.ones((vop.shape[0], HEAD), BF)

    def _row(self, dy):
        return (self.me.y + dy) % 4

    def _sums(self, m):
        a = self.buf["acc"][m]
        return a[:, :HEAD], jnp.transpose(a[:, HEAD:])[:8]

    def _post(self, k, m, dst, slot, where, kind):
        b, s = self.buf, self.sem
        big, small = ("od", "dd") if kind == 1 else ("ro", "rd")
        remote(b["ob"].at[m], b[big].at[dst], s["o_out"].at[0, k], s["o_in"].at[kind, 0, slot], where).start()
        remote(b["db"].at[m], b[small].at[dst], s["o_out"].at[1, k], s["o_in"].at[kind, 1, slot], where).start()

    def send_far_sums(self):
        me, b = self.me, self.buf
        for c, dy in ((0, 1), (1, 3)):
            m = self._row(2) * 2 + c
            o, d = self._sums(m)
            b["ob"][m] = o.astype(BF)
            b["db"][m] = d
            self._post(c, m, c, c, (me.z, self._row(dy), me.c, me.t), 0)

    def send_sums(self):
        me, b, s = self.me, self.buf, self.sem
        for c in (0, 1):
            await_bytes(b["ro"].at[c], s["o_in"].at[0, 0, c])
            await_bytes(b["rd"].at[c], s["o_in"].at[0, 1, c])
        for side, dy in ((0, 1), (1, 3)):
            for c in (0, 1):
                m = self._row(dy) * 2 + c
                o, d = self._sums(m)
                if c == side:
                    o = o + b["ro"][side].astype(F32)
                    d = d + b["rd"][side]
                b["ob"][m] = o.astype(BF)
                b["db"][m] = d
                into = 2 * side + me.c
                self._post(2 + 2 * side + c, m, into, into, (me.z, self._row(dy), c, me.t), 1)
        m = me.y * 2 + 1 - me.c
        o, d = self._sums(m)
        b["ob"][m] = o.astype(BF)
        b["db"][m] = d
        self._post(6, m, 4 + me.c, 4 + me.c, (me.z, me.y, 1 - me.c, me.t), 1)
        o, d = self._sums(me.s8)
        b["od"][4 + me.c] = o.astype(BF)
        b["dd"][4 + me.c] = d

    def finish(self):
        b, s = self.buf, self.sem
        od, dd = b["od"], b["dd"]
        out_gain = self.ins[9]
        for k in range(4):
            await_bytes(od.at[k], s["o_in"].at[1, 0, k])
            await_bytes(dd.at[k], s["o_in"].at[1, 1, k])
        await_bytes(od.at[0], s["o_in"].at[1, 0, 5 - self.me.c])
        await_bytes(dd.at[0], s["o_in"].at[1, 1, 5 - self.me.c])
        for h in (0, 1):
            o = sum(od[2 * y + h].astype(F32) for y in range(3))
            d = sum(dd[2 * y + h] for y in range(3))
            den = jnp.transpose(jnp.broadcast_to(d[0:1], (HEAD, d.shape[1])))
            m = o / den
            m = m * lax.rsqrt(jnp.mean(m * m, axis=-1, keepdims=True) + EPS) * out_gain[...]
            self.out[:, HEAD * h : HEAD * (h + 1)] = m.astype(BF)

    def drain(self):
        b, s = self.buf, self.sem
        await_bytes(b["kvb"].at[0], s["kv_out"].at[0])
        await_bytes(b["rkb"], s["kv_out"].at[1])
        await_bytes(b["q_all"].at[pl.ds(0, SRC - 1)], s["q_out"])
        for slot, up in [(k, True) for k in range(UP)] + [(0, False)] + [(UP + k, False) for k in range(1, DOWN)]:

            @pl.when(self.sends(slot, up))
            def _():
                for copy in self._copies(slot, up):
                    copy.wait_send()

        for k in range(7):
            await_bytes(b["ob"].at[0], s["o_out"].at[0, k])
            await_bytes(b["db"].at[0], s["o_out"].at[1, k])


ATT_BUFS = {
    "kv": ((8, 512, 256), "bf"),
    "rk": ((8, 256, 128), "bf"),
    "kvb": ((2, 256, 256), "bf"),
    "rkb": ((128, 128), "bf"),
    "q_all": ((8, 256, 256), "bf"),
    "qb": ((2, 256, 256), "bf"),
    "acc": ((8, 256, 256), "f"),
    "kop": ((512, 256), "bf"),
    "vop": ((512, 256), "bf"),
    "ob": ((8, 256, 128), "bf"),
    "db": ((8, 8, 256), "f"),
    "od": ((6, 256, 128), "bf"),
    "dd": ((6, 8, 256), "f"),
    "ro": ((2, 256, 128), "bf"),
    "rd": ((2, 8, 256), "f"),
}
ATT_SEMS = {"kv_out": (2,), "kv_in": (8,), "rk_in": (8,), "q_out": None, "q_in": None, "hop_out": (8, 2), "o_out": (2, 7), "o_in": (2, 2, 6)}


def att_scratch():
    bufs = [pltpu.VMEM(shape, BF if kind == "bf" else F32) for shape, kind in ATT_BUFS.values()]
    sems = [pltpu.SemaphoreType.DMA if n is None else pltpu.SemaphoreType.DMA(n) for n in ATT_SEMS.values()]
    return bufs + sems


def att_refs(refs):
    n = len(ATT_BUFS)
    return dict(zip(ATT_BUFS, refs[:n])), dict(zip(ATT_SEMS, refs[n:]))


BIG = ("tokens", "queries", "kv_latent", "w_key", "w_val", "near", "un_main", "un_extra", "pk_main", "pk_extra")
OWN = (
    "wgu",
    "wd",
    "normed",
    "outb",
    "arr",
    "rows",
    "hid",
    "wmix",
    "far",
    "to_r",
    "to_l",
    "relay",
    "from_l",
    "from_r",
    "retb",
    "reti",
    "fino",
    "fini",
    "w_sem",
    "own_sem",
    "out_sem",
    "xs_sem",
    "xr_sem",
    "rs_send",
    "relay_sem",
    "fl_sem",
    "fr_sem",
    "ret_send",
    "ret_sem",
    "fin_send",
    "fin_sem",
)


def whole_kernel(n_z, *refs):
    n_small, n_big, n_own = 10, len(BIG), len(OWN)
    (lat_gain, q_gain, key_gain, rope_gain, out_gain, far_table, rope_key, gain, routes_t, weights_t) = refs[:n_small]
    refs = refs[n_small:]
    big_hbm, (wg_hbm, wu_hbm, wd_hbm), refs = refs[:n_big], refs[n_big : n_big + 3], refs[n_big + 3 :]
    a_out, out, refs = refs[0], refs[1], refs[2:]
    own = dict(zip(OWN, refs[:n_own]))
    big, big_sem, refs = refs[n_own : n_own + n_big], refs[n_own + n_big], refs[n_own + n_big + 1 :]
    (tokens, queries, kv_latent, w_key, w_val, near_table, un_main, un_extra, pk_main, pk_extra) = big
    takes = [pltpu.make_async_copy(h, v, big_sem.at[k]) for k, (h, v) in enumerate(zip(big_hbm, big))]
    for take in takes:
        take.start()
    a_in = (queries, kv_latent, rope_key, lat_gain, w_key, w_val, q_gain, key_gain, rope_gain, out_gain, near_table, far_table)
    wgu, wd, normed, outb, arr, rows = (own[k] for k in ("wgu", "wd", "normed", "outb", "arr", "rows"))
    hid, wmix, far, to_r, to_l, relay = (own[k] for k in ("hid", "wmix", "far", "to_r", "to_l", "relay"))
    from_l, from_r, retb, reti, fino, fini = (own[k] for k in ("from_l", "from_r", "retb", "reti", "fino", "fini"))
    w_sem, own_sem, out_sem, xs_sem, xr_sem, rs_send = (own[k] for k in ("w_sem", "own_sem", "out_sem", "xs_sem", "xr_sem", "rs_send"))
    relay_sem, fl_sem, fr_sem, ret_send, ret_sem, fin_send = (own[k] for k in ("relay_sem", "fl_sem", "fr_sem", "ret_send", "ret_sem", "fin_send"))
    fin_sem = own["fin_sem"]
    me = Place(n_z)
    att = Attention(n_z, me, a_in, a_out, *att_refs(refs))
    greet(me, n_z)
    ff = wd.shape[0]
    loads = [
        pltpu.make_async_copy(wg_hbm.at[0], wgu.at[:, pl.ds(0, ff)], w_sem.at[0]),
        pltpu.make_async_copy(wu_hbm.at[0], wgu.at[:, pl.ds(ff, ff)], w_sem.at[1]),
        pltpu.make_async_copy(wd_hbm.at[0], wd, w_sem.at[2]),
    ]
    for load in loads:
        load.start()
    n_rows, model = tokens.shape
    cols = model // 4
    quarter = n_rows // 4

    exp_ids = lax.broadcasted_iota(I32, (64, n_rows), 0)
    ra, rb = routes_t[0:1, :], routes_t[1:2, :]
    hit_a, hit_b = exp_ids == ra, exp_ids == rb
    both = jnp.where(hit_a | hit_b, 1.0, 0.0).astype(BF)
    i0 = lax.broadcasted_iota(I32, (n_rows, n_rows), 0)
    i1 = lax.broadcasted_iota(I32, (n_rows, n_rows), 1)
    same = (i0 // quarter) == (i1 // quarter)
    earlier_t = jnp.where((i0 < i1) & same, 1.0, 0.0).astype(BF)
    count_t = dot(both, earlier_t)
    base_t = lax.broadcasted_iota(I32, (1, n_rows), 1) // quarter * 3

    def places(hit, chosen):
        s = base_t + jnp.sum(jnp.where(hit, count_t, 0.0), axis=0, keepdims=True).astype(I32)
        return chosen * MSG + s, chosen * MSG + CAP + s % 4 + 2048 * (s // 4)

    (ma, xa), (mb, xb) = places(hit_a, ra), places(hit_b, rb)

    takes[0].wait()
    v = tokens[...].astype(F32)
    scale = lax.rsqrt(jnp.mean(v * v, axis=-1, keepdims=True) + EPS)
    mine = pl.ds(pl.multiple_of(me.t * cols, cols), cols)
    normed[...] = (tokens[:, mine].astype(F32) * scale * gain[:, mine]).astype(BF)

    met(n_z)

    def dispatch(o, _):
        z = (me.z + me.row(o)) % n_z
        first = z * SRC * MSG
        ids = lax.broadcasted_iota(I32, (SRC * MSG, n_rows), 0) + first
        main = jnp.where((ids == ma) | (ids == mb), 1.0, 0.0).astype(BF)
        block = dot(main, normed[:, : 3 * 128])
        extra = []
        for j in range(3):
            idj = ids + 2048 * j
            sel = jnp.where((idj == xa) | (idj == xb), 1.0, 0.0).astype(BF)
            extra.append(dot(sel, normed[:, 3 * 128 :]))
        block = block + jnp.concatenate(extra, axis=1)
        outb[o] = block.astype(BF).reshape(SRC, MSG, 3 * 128)

        def send(i, _):
            s = (me.s8 + i) % SRC
            remote(outb.at[o, s], arr.at[0, o, me.s8], out_sem, own_sem.at[o], me.at(z, s)).start()
            return 0

        lax.fori_loop(jnp.where(o == 0, 1, 0), SRC, send, 0)
        return 0

    lax.fori_loop(0, n_z, dispatch, 0)
    pltpu.make_async_copy(outb.at[0, me.s8], arr.at[0, 0, me.s8], own_sem.at[0]).start()

    upright = lambda row: jnp.transpose(jnp.broadcast_to(row, (128, n_rows)))[:, 0:1]
    lane_e = lax.broadcasted_iota(I32, (n_rows, 128), 1)
    ca, cb = (upright(r.astype(F32)).astype(I32) for r in (ra, rb))
    on_a, on_b = lane_e == ca, lane_e == cb
    earlier = jnp.where((i1 < i0) & same, 1.0, 0.0).astype(BF)
    count = dot(earlier, jnp.where(on_a | on_b, 1.0, 0.0).astype(BF))
    base = lax.broadcasted_iota(I32, (n_rows, 1), 0) // quarter * 3
    wa, wb = (upright(weights_t[k : k + 1, :]) for k in (0, 1))

    def places_c(hit, chosen):
        s = base + jnp.sum(jnp.where(hit, count, 0.0), axis=1, keepdims=True).astype(I32)
        return chosen * MSG + s, chosen * MSG + CAP + s % 4 + 2048 * (s // 4)

    (cma, cxa), (cmb, cxb) = places_c(on_a, ca), places_c(on_b, cb)

    def mix(k, _):
        lanes = lax.broadcasted_iota(I32, (n_rows, 64 * MSG), 1)
        idk = lanes + 2048 * (k - 1)
        pa, pb = jnp.where(k == 0, cma - 2048, cxa), jnp.where(k == 0, cmb - 2048, cxb)
        w = jnp.where(idk == pa, wa, 0.0) + jnp.where(idk == pb, wb, 0.0)
        hi, lo = split_two(w)
        wmix[k, 0] = hi
        wmix[k, 1] = lo
        return 0


    def pass_on(b, o, step, dst):
        remote(arr.at[b, o], arr.at[dst, o], xs_sem.at[b, step % 4 // 2], xr_sem.at[dst - 1, o], me.x(step)).start()

    def rank_cols(rank, width=cols, skip=0):
        return pl.ds(pl.multiple_of((me.t + rank) % 4 * cols + skip, 128), width)

    def unpack(b, rank, p):
        packed = arr[b, pl.ds(2 * p, 2)].reshape(2 * SRC * MSG, 3 * 128)
        tiles = jnp.concatenate([packed[:, 128 * j : 128 * (j + 1)] for j in range(3)], axis=0)
        rows[:, rank_cols(rank, 3 * 128)] = dot(un_main[...], packed).astype(BF)
        rows[:, rank_cols(rank, 128, 3 * 128)] = dot(un_extra[...], tiles).astype(BF)

    def unpack_near(p):
        for b, rank in ((0, 0), (1, 3), (2, 1)):
            unpack(b, rank, p)

    def gather(o):
        await_bytes(arr.at[0, o], own_sem.at[o])
        pass_on(0, o, 1, 1)
        pass_on(0, o, 3, 2)

    def relay_on(o):
        await_bytes(arr.at[1, o], xr_sem.at[0, o])
        await_bytes(arr.at[2, o], xr_sem.at[1, o])

        @pl.when(o % 2 == 0)
        def _():
            pass_on(1, o, 1, 3)

        @pl.when(o % 2 == 1)
        def _():
            pass_on(2, o, 3, 3)

    def down(q, rank):
        return dot(hid[q], wd[:, rank_cols(rank)])

    half = 96
    parts = (pl.ds(0, half), pl.ds(half, half))

    def hidden_units(p):
        await_bytes(arr.at[3, 2 * p], xr_sem.at[2, 2 * p])
        await_bytes(arr.at[3, 2 * p + 1], xr_sem.at[2, 2 * p + 1])
        unpack(3, 2, p)
        gu = dot(rows[...], wgu[...])
        g, u = gu[:, :ff], gu[:, ff:]
        hid[p] = (g / (1.0 + jnp.exp(-g)) * u).astype(BF)
        far[p] = down(p, 2).astype(BF)
        for k, step in ((0, 1), (1, 3)):
            remote(far.at[p, parts[k]], relay.at[p, parts[k]], rs_send.at[0, p, k], relay_sem.at[p, k], me.x(step)).start()

    ways = ((to_r, from_l, fl_sem, 1), (to_l, from_r, fr_sem, 3))

    def half_down(q, rank, h):
        return dot(hid[q, parts[h]], wd[:, rank_cols(rank)])

    def send_half(q, k, h, y):
        buf, dst, sem, rank = ways[k]
        buf[q, parts[h]] = y.astype(BF)
        remote(buf.at[q, parts[h]], dst.at[q, parts[h]], rs_send.at[1 + k, q, h], sem.at[q, h], me.x(rank)).start()

    def own_halves(q):
        for k in (0, 1):
            send_half(q, k, 1 - k, half_down(q, ways[k][3], 1 - k))

    def sides(q):
        for k in (0, 1):
            y = half_down(q, ways[k][3], k)
            await_bytes(relay.at[q, parts[k]], relay_sem.at[q, k])
            send_half(q, k, k, y + relay[q, parts[k]].astype(F32))

    def finish(q):
        y = down(q, 0)
        for h in (0, 1):
            await_bytes(from_l.at[q, parts[h]], fl_sem.at[q, h])
            await_bytes(from_r.at[q, parts[h]], fr_sem.at[q, h])
        y = (y + from_l[q].astype(F32) + from_r[q].astype(F32)).astype(BF)
        ext = dot(pk_extra[...], y[:, 3 * 128 :])
        packed = dot(pk_main[...], y[:, : 3 * 128]) + jnp.concatenate([ext[256 * j : 256 * (j + 1)] for j in range(3)], axis=1)
        retb[pl.ds(2 * q, 2)] = packed.astype(BF).reshape(2, SRC, MSG, 3 * 128)
        mine_e = me.z * SRC + me.s8

        def send(i, _):
            o = 2 * q + i // SRC
            z = (me.z - me.row(o) + n_z) % n_z
            s = (me.s8 + i) % SRC
            remote(retb.at[o, s], reti.at[mine_e], ret_send, ret_sem, me.at(z, s)).start()
            return 0

        lax.fori_loop(jnp.where(q == 0, 1, 0), 2 * SRC, send, 0)

        @pl.when(q == 0)
        def _():
            pltpu.make_async_copy(retb.at[0, me.s8], reti.at[mine_e], ret_sem).start()

    n_pairs = n_z // 2

    def step(k, _):
        @pl.when(k < n_pairs)
        def _():
            gather(2 * k)

            @pl.when(k == 0)
            def _():
                for take in takes[1:]:
                    take.wait()
                att.prepare()
                att.ones()
                att.send_first()
                lax.fori_loop(0, 4, mix, 0)

            @pl.when(k > 0)
            def _():
                relay_on(2 * k - 1)
                unpack_near(k - 1)

            gather(2 * k + 1)
            relay_on(2 * k)

        @pl.when(k == n_pairs)
        def _():
            relay_on(n_z - 1)
            unpack_near(n_pairs - 1)

        @pl.when(k == QUERY_AT)
        def _():
            att.send_queries()

        @pl.when(k == HOP_AT)
        def _():
            att.first_in()
            att.hop(0, True)
            att.hop(0, False)

        last = jnp.where(me.z > DOWN - 1, PAIR_AT + DOWN - 1, jnp.where(me.z == 0, FIRST_AT, PAIR_AT + me.z - 1))

        @pl.when((k >= PAIR_AT) & (k < PAIR_AT + DOWN))
        def _():
            att.pairs(k - PAIR_AT + 1, False)

        @pl.when((k >= 2) & (k < n_pairs + 2))
        def _():
            sides(k - 2)

        @pl.when((k >= 3) & (k < n_pairs + 3))
        def _():
            finish(k - 3)

        @pl.when((k >= 1) & (k < n_pairs + 1))
        def _():
            @pl.when(k == 1)
            def _():
                loads[0].wait()
                loads[1].wait()
                loads[2].wait()

            hidden_units(k - 1)
            own_halves(k - 1)

        @pl.when(k == FIRST_AT)
        def _():
            att.queries_in()
            att.attend(0, True)

        @pl.when((k >= PAIR_AT) & (k < PAIR_AT + DOWN))
        def _():
            att.pairs(k - PAIR_AT + 1, True)

        @pl.when(k == last)
        def _():
            att.send_far_sums()

        @pl.when(k == last + 1)
        def _():
            att.send_sums()

        return 0

    lax.fori_loop(0, n_pairs + 3, step, 0)
    att.finish()

    await_bytes(reti, ret_sem)
    res = reti[...].reshape(64 * MSG, 3 * 128)
    mixed = dot(wmix[0, 0], res) + dot(wmix[0, 1], res)
    last = jnp.zeros((n_rows, 128), F32)
    for j in range(3):
        piece = res[:, 128 * j : 128 * (j + 1)]
        last = last + dot(wmix[1 + j, 0], piece) + dot(wmix[1 + j, 1], piece)
    fino[:, :, : 3 * 128] = mixed.astype(BF).reshape(4, quarter, 3 * 128)
    fino[:, :, 3 * 128 :] = last.astype(BF).reshape(4, quarter, 128)
    for step in (1, 2, 3):
        remote(fino.at[(me.t + step) % 4], fini.at[step - 1], fin_send.at[step - 1], fin_sem.at[step - 1], me.x(step)).start()
    out[:, mine] = fino[me.t]
    for step in (1, 2, 3):
        await_bytes(fini.at[step - 1], fin_sem.at[step - 1])
        theirs = pl.ds(pl.multiple_of((me.t + 4 - step) % 4 * cols, cols), cols)
        out[:, theirs] = fini[step - 1]

    for step in (0, 1, 2):
        await_bytes(fini.at[step], fin_send.at[step])
    for q in range(4):
        for k in (0, 1):
            await_bytes(far.at[q, parts[k]], rs_send.at[0, q, k])
            for h in (0, 1):
                await_bytes(far.at[q, parts[h]], rs_send.at[1 + k, q, h])
    for b, k, n in ((0, 0, n_z), (0, 1, n_z), (1, 0, n_z // 2), (2, 1, n_z // 2)):
        await_bytes(arr.at[b, pl.ds(0, n)], xs_sem.at[b, k])
    for buf, sem in ((outb, out_sem), (retb, ret_send)):
        await_bytes(buf.at[pl.ds(1, n_z - 1)], sem)
        await_bytes(buf.at[0, pl.ds(1, SRC - 1)], sem)
    att.drain()


NEAR = 256


def rope_constants(n_places):
    freqs = 1.0 / THETA ** (np.arange(0, ROPE, 2, dtype=np.float64) / ROPE)
    freqs = np.tile(freqs.astype(np.float32).astype(np.float64), 4)
    table = lambda at: jnp.asarray(np.stack([np.cos(at[:, None] * freqs), np.sin(at[:, None] * freqs)]), F32)
    return table(np.arange(NEAR)), table(np.arange(n_places) * NEAR)


def settle(results):
    count = len(results)

    def body(*refs):
        src, dst, held, sem = refs[:count], refs[count : 2 * count], refs[2 * count : 3 * count], refs[3 * count]
        ins = [pltpu.make_async_copy(a, b, sem.at[0, k]) for k, (a, b) in enumerate(zip(src, held))]
        outs = [pltpu.make_async_copy(a, b, sem.at[1, k]) for k, (a, b) in enumerate(zip(held, dst))]
        for copy in ins:
            copy.start()
        for taken, copy in zip(ins, outs):
            taken.wait()
            copy.start()
        for copy in outs:
            copy.wait()

    hbm = pl.BlockSpec(memory_space=pl.ANY)
    return pl.pallas_call(
        body,
        out_shape=tuple(jax.ShapeDtypeStruct(a.shape, a.dtype) for a in results),
        in_specs=[hbm] * count,
        out_specs=(hbm,) * count,
        scratch_shapes=[pltpu.VMEM(a.shape, a.dtype) for a in results] + [pltpu.SemaphoreType.DMA((2, count))],
        name="settle",
    )(*results)


def on_device(
    queries,
    kv_latent,
    rope_key,
    latent_gain,
    w_key_up,
    w_value_up,
    query_gain,
    key_gain,
    rope_gain,
    out_gain,
    moe_tokens,
    moe_gain,
    routes,
    route_weights,
    w_gate,
    w_up,
    w_down,
):
    n_z = lax.axis_size("ep_0")
    n_rows, model = moe_tokens.shape
    ff = w_gate.shape[2]
    cols = model // 4
    row = lambda g: g.reshape(1, -1)
    vm = pl.BlockSpec(memory_space=pltpu.VMEM)
    hbm = pl.BlockSpec(memory_space=pl.ANY)
    chunk = (4, 192, cols)
    near, far = rope_constants(n_z * SRC)
    small = tuple(row(g) for g in (latent_gain, query_gain, key_gain, rope_gain, out_gain))
    small += (far, rope_key.T, row(moe_gain), routes.T, route_weights.T)
    big = (moe_tokens, queries, kv_latent, w_key_up, w_value_up, near, *fixed_selects())
    dma = pltpu.SemaphoreType.DMA
    results = pl.pallas_call(
        functools.partial(whole_kernel, n_z),
        out_shape=(
            jax.ShapeDtypeStruct((n_rows, 2 * HEAD), BF),
            jax.ShapeDtypeStruct((n_rows // 4, model), BF),
        ),
        in_specs=[vm] * len(small) + [hbm] * (len(big) + 3),
        out_specs=(vm, vm),
        scratch_shapes=[
            pltpu.VMEM((model, 2 * ff), BF),
            pltpu.VMEM((ff, model), BF),
            pltpu.VMEM((n_rows, cols), BF),
            pltpu.VMEM((n_z, SRC, MSG, 384), BF),
            pltpu.VMEM((4, n_z, SRC, MSG, 384), BF),
            pltpu.VMEM((192, model), BF),
            pltpu.VMEM((4, 192, ff), BF),
            pltpu.VMEM((4, 2, n_rows, 64 * MSG), BF),
            *[pltpu.VMEM(chunk, BF)] * 6,
            pltpu.VMEM((n_z, SRC, MSG, 384), BF),
            pltpu.VMEM((n_z * SRC, MSG, 384), BF),
            pltpu.VMEM((4, n_rows // 4, cols), BF),
            pltpu.VMEM((3, n_rows // 4, cols), BF),
            dma((3,)),
            dma((n_z,)),
            dma,
            dma((3, 2)),
            dma((3, n_z)),
            dma((3, 4, 2)),
            dma((4, 2)),
            dma((4, 2)),
            dma((4, 2)),
            dma,
            dma,
            dma((3,)),
            dma((3,)),
            *[pltpu.VMEM(a.shape, a.dtype) for a in big],
            dma((len(big),)),
            *att_scratch(),
        ],
        compiler_params=pltpu.CompilerParams(collective_id=1, has_side_effects=True, vmem_limit_bytes=62 * 1024 * 1024),
        name="layer",
    )(
        *small,
        *big,
        w_gate,
        w_up,
        w_down,
    )
    return settle(results)


def solution(mesh):
    finer = Mesh(mesh.devices.reshape(8, 4, 2, mesh.shape["tp"]), ("ep_0", "ep_1", "ep_2", "tp"))
    placed = (
        P(EP, "tp"),
        P(EP, None),
        P(EP, None),
        P(),
        P(None, "tp"),
        P(None, "tp"),
        P(),
        P(),
        P(),
        P(),
        P(EP, None),
        P(),
        P(EP, None),
        P(EP, None),
        P(EP, None, "tp"),
        P(EP, None, "tp"),
        P(EP, "tp", None),
    )
    return jax.shard_map(
        on_device,
        mesh=finer,
        in_specs=placed,
        out_specs=(P(EP, "tp"), P(EP_TP, None)),
        check_vma=False,
    )
```
